32 devices in a mesh: sp: 16 (over z, y, core), fs: 1, tp: 2 (over x).
Axes of the slice: x: 2, y: 2, z: 4, core: 2. Of those that a mesh axis runs over, the one named last changes fastest.
Arguments:
- tokens: bfloat16 [1, 4096, 2048], P('fs', 'sp'), may hold values from -6 to 6
- norm_gain: float32 [2048], replicated, may hold values from 0.1 to 1.9
- w_state_in: bfloat16 [2048, 1024], P(('sp', 'fs'), 'tp'), may hold values from -0.125 to 0.125
- w_value: bfloat16 [2048, 1024], P(('sp', 'fs'), 'tp'), may hold values from -0.125 to 0.125
- w_outer: bfloat16 [2048, 1024], P(('sp', 'fs'), 'tp'), may hold values from -0.125 to 0.125
- w_inner: bfloat16 [2048, 1024], P(('sp', 'fs'), 'tp'), may hold values from -0.125 to 0.125
- w_state_out: bfloat16 [2048, 1024], P(('sp', 'fs'), 'tp'), may hold values from -0.125 to 0.125
- w_conv_out: bfloat16 [2048, 1024], P(('sp', 'fs'), 'tp'), may hold values from -0.125 to 0.125
- log_step: float32 [64], P('tp'), may hold values from -4.6 to -3.2
- decay_real: float32 [64, 64], P('tp'), may hold values from -5 to 0
- frequency: float32 [64, 64], P('tp'), may hold values from 1 to 192
- step_rate: float32 [1, 4096], P('fs', 'sp'), may hold values from 0.4 to 2.5
- input_real: float32 [64, 64, 16], P('tp'), may hold values from -1 to 1
- input_imag: float32 [64, 64, 16], P('tp'), may hold values from -1 to 1
- read_real: float32 [64, 16, 64], P('tp'), may hold values from -0.75 to 0.75
- read_imag: float32 [64, 16, 64], P('tp'), may hold values from -0.75 to 0.75
- skip_gain: float32 [64, 16], P('tp'), may hold values from -4 to 4
- conv_taps: float32 [3, 1024], P(None, 'tp'), may hold values from -3.5 to 3.5
- initial_state: float32 [1, 2, 64, 64], P('fs', None, 'tp'), may hold values from -6 to 6
Outputs:
- mixed: bfloat16 [1, 4096, 2048], P('fs', ('sp', 'tp'))
- final_state: float32 [1, 2, 64, 64], P('fs', None, 'tp', 'sp')
The draws below stay inside these ranges and needn't reach their ends.
All inputs are finite; a program needn't handle non-finite values.
Results may differ from the reference program's by a relative error of at most 0.018.
Values may be sent and summed in bfloat16 or wider, within the bound.
A program may use at most 64 MiB of HBM per device.

```python
import math
import jax
import jax.numpy as jnp
from jax import lax

D = 2048
GROUPS = 64
GROUP = 16
STATE = 64
CW = 1024
KW = 3
SW = 1024
SEQS = 1
LENGTH = 4096
N_TP = 2


def draw_decay_real(key, part):
    base = jax.random.fold_in(key, 7)
    key_pick, key_slow, key_fast = jax.random.split(base, 3)
    share = 0.5
    pick = jax.random.uniform(key_pick, (GROUPS, 1), jnp.float32) < share
    slow = -jnp.exp(jax.random.uniform(key_slow, (GROUPS, STATE), jnp.float32, math.log(5.0 / LENGTH), math.log(60.0 / LENGTH)))
    fast = -jnp.exp(jax.random.uniform(key_fast, (GROUPS, STATE), jnp.float32, math.log(2.0), math.log(5.0)))
    return jnp.where(pick, slow, fast)


def draw_step_rate(key, part):
    base = jax.random.fold_in(key, 13)
    key_slow, key_fine = jax.random.split(base, 2)
    blocks = LENGTH // 256
    slow = jnp.exp(jax.random.uniform(key_slow, (SEQS, blocks), jnp.float32, math.log(0.5), math.log(2.0)))
    fine = jax.random.uniform(key_fine, (SEQS, LENGTH), jnp.float32, 0.8, 1.25)
    return jnp.repeat(slow, 256, axis=1) * fine


def shard_levels(own_key, shape, cuts, smallest, top_value):
    level, own = 1.0, jax.random.fold_in(own_key, 6)
    for axis_at, parts in cuts:
        draws = jnp.exp(jax.random.uniform(jax.random.fold_in(own, axis_at), (parts,), jnp.float32, smallest / len(cuts), top_value / len(cuts)))
        level = level * jnp.repeat(draws, shape[axis_at] // parts).reshape([-1 if axis == axis_at else 1 for axis in range(len(shape))])
    return level


def noise(rng, shape, deviation, reach, pieces=(), kind=jnp.bfloat16):
    drawn = jax.random.normal(rng, shape, jnp.float32) * deviation
    if len(pieces) > 0:
        drawn = shard_levels(rng, shape, pieces, -0.22, 0.18) * drawn
    return jnp.clip(drawn, min=-reach, max=reach).astype(kind)


def setup_inputs(seed: int = 0) -> dict:
    streams_of = jax.random.split(jax.random.key(seed), 20)
    return {
        "tokens": noise(streams_of[0], (SEQS, LENGTH, D), 1.0, 6.0, ((1, 16),)),
        "norm_gain": jnp.clip(1.0 + 0.18 * jax.random.normal(streams_of[1], (D,), jnp.float32), 0.1, 1.9),
        "w_state_in": noise(streams_of[2], (D, SW), D ** -0.5, 0.125, ((0, 16), (1, 2))),
        "w_value": noise(streams_of[3], (D, CW), D ** -0.5, 0.125, ((0, 16), (1, 2))),
        "w_outer": noise(streams_of[4], (D, CW), D ** -0.5, 0.125, ((0, 16), (1, 2))),
        "w_inner": noise(streams_of[5], (D, CW), D ** -0.5, 0.125, ((0, 16), (1, 2))),
        "w_state_out": noise(streams_of[6], (D, SW), (SW + CW) ** -0.5, 0.125, ((0, 16), (1, 2))),
        "w_conv_out": noise(streams_of[7], (D, CW), (SW + CW) ** -0.5, 0.125, ((0, 16), (1, 2))),
        "log_step": jnp.clip(-4.6 + 1.3999999 * jax.random.uniform(streams_of[8], (GROUPS,), jnp.float32) ** shard_levels(streams_of[8], (GROUPS,), ((0, 2),), -0.2, 0.2), -4.6, -3.2),
        "decay_real": draw_decay_real(jax.random.fold_in(streams_of[19], 71), 0),
        "frequency": jnp.clip(1.0 + 191.0 * jax.random.uniform(streams_of[10], (GROUPS, STATE), jnp.float32) ** shard_levels(streams_of[10], (GROUPS, STATE), ((0, 2),), -0.2, 0.2), 1.0, 192.0),
        "step_rate": draw_step_rate(jax.random.fold_in(streams_of[19], 71), 0),
        "input_real": noise(streams_of[12], (GROUPS, STATE, GROUP), (2 * GROUP) ** -0.5, 1.0, ((0, 2),), jnp.float32),
        "input_imag": noise(streams_of[13], (GROUPS, STATE, GROUP), (2 * GROUP) ** -0.5, 1.0, ((0, 2),), jnp.float32),
        "read_real": noise(streams_of[14], (GROUPS, GROUP, STATE), STATE ** -0.5, 0.75, ((0, 2),), jnp.float32),
        "read_imag": noise(streams_of[15], (GROUPS, GROUP, STATE), STATE ** -0.5, 0.75, ((0, 2),), jnp.float32),
        "skip_gain": noise(streams_of[16], (GROUPS, GROUP), 1.0, 4.0, ((0, 2),), jnp.float32),
        "conv_taps": noise(streams_of[17], (KW, CW), KW ** -0.5, 3.5, ((1, 2),), jnp.float32),
        "initial_state": noise(streams_of[18], (SEQS, 2, GROUPS, STATE), 1.0, 6.0, ((2, 2),), jnp.float32),
    }


def reference(tokens, norm_gain, w_state_in, w_value, w_outer, w_inner, w_state_out, w_conv_out, log_step, decay_real, frequency, step_rate, input_real, input_imag, read_real, read_imag, skip_gain, conv_taps, initial_state):
    seqs, length, width = tokens.shape
    features = tokens.astype(jnp.float32)
    mean_square = lax.optimization_barrier(jnp.mean(features * features, axis=-1, keepdims=True))
    normed = (features * lax.rsqrt(mean_square + 1e-06) * norm_gain).astype(jnp.bfloat16).reshape(seqs * length, width)

    def project(matrix):
        return jnp.dot(normed, matrix, preferred_element_type=jnp.float32).astype(jnp.bfloat16)
    state_in = project(w_state_in)
    value = project(w_value)
    outer = project(w_outer)
    inner = project(w_inner)
    groups, states = decay_real.shape
    group = skip_gain.shape[1]
    channels = state_in.astype(jnp.float32).reshape(seqs, length, groups, group)
    step = jnp.exp(log_step)[None, None, :] * step_rate[:, :, None]
    modulus = decay_real * decay_real + frequency * frequency

    def advance(carry, inputs):
        hidden_real, hidden_imag = carry
        chan_now, step_now = inputs
        scaled = step_now[..., None]
        grow = jnp.exp(scaled * decay_real)
        angle = scaled * frequency
        bar_real = grow * jnp.cos(angle)
        bar_imag = grow * jnp.sin(angle)
        less_real = bar_real - 1.0
        hold_real = (less_real * decay_real + bar_imag * frequency) / modulus
        hold_imag = (bar_imag * decay_real - less_real * frequency) / modulus
        drive_real = jnp.einsum('sgh,gph->sgp', chan_now, input_real, precision=lax.Precision.HIGHEST)
        drive_imag = jnp.einsum('sgh,gph->sgp', chan_now, input_imag, precision=lax.Precision.HIGHEST)
        push_real = hold_real * drive_real - hold_imag * drive_imag
        push_imag = hold_real * drive_imag + hold_imag * drive_real
        next_real = bar_real * hidden_real - bar_imag * hidden_imag + push_real
        next_imag = bar_real * hidden_imag + bar_imag * hidden_real + push_imag
        response = jnp.einsum('sgp,ghp->sgh', next_real, read_real, precision=lax.Precision.HIGHEST) - jnp.einsum('sgp,ghp->sgh', next_imag, read_imag, precision=lax.Precision.HIGHEST) + skip_gain * chan_now
        return ((next_real, next_imag), response)
    (last_real, last_imag), responses = lax.scan(advance, (initial_state[:, 0], initial_state[:, 1]), (channels.transpose(1, 0, 2, 3), step.transpose(1, 0, 2)))
    state_mix = jax.nn.gelu(responses.transpose(1, 0, 2, 3)).reshape(seqs * length, groups * group).astype(jnp.bfloat16)
    final_state = jnp.stack([last_real, last_imag], axis=1)
    gated = (inner.astype(jnp.float32) * value.astype(jnp.float32)).astype(jnp.bfloat16).reshape(seqs, length, -1)
    taps = conv_taps.shape[0]
    padded = jnp.pad(gated, ((0, 0), (taps - 1, 0), (0, 0))).astype(jnp.float32)
    filtered = jnp.zeros((seqs, length, gated.shape[2]), jnp.float32)
    for tap in range(taps):
        filtered = filtered + conv_taps[tap] * padded[:, tap:tap + length]
    conv_mix = (outer.astype(jnp.float32).reshape(seqs, length, -1) * filtered).astype(jnp.bfloat16).reshape(seqs * length, -1)
    state_block = state_mix.shape[1] // N_TP
    conv_block = conv_mix.shape[1] // N_TP
    total = jnp.zeros((seqs * length, width), jnp.float32)
    for block in range(N_TP):
        part = jnp.dot(state_mix[:, block * state_block:(block + 1) * state_block], w_state_out[:, block * state_block:(block + 1) * state_block].T, preferred_element_type=jnp.float32) + jnp.dot(conv_mix[:, block * conv_block:(block + 1) * conv_block], w_conv_out[:, block * conv_block:(block + 1) * conv_block].T, preferred_element_type=jnp.float32)
        total = total + lax.optimization_barrier(part.astype(jnp.bfloat16)).astype(jnp.float32)
    mixed = total.astype(jnp.bfloat16).reshape(seqs, length, width)
    return (mixed, final_state)
```

```python
import math

import jax
import jax.numpy as jnp
from jax import lax
from jax.experimental import pallas as pl
from jax.experimental.pallas import tpu as pltpu
from jax.sharding import PartitionSpec as P

F32 = jnp.float32
BF16 = jnp.bfloat16
SUB = 8
SIN = (3.1415925798055846, -5.16770686616794, 2.5500311935192803, -0.5980441939118888, 0.07721838615680923)
COS = (0.9999999997799038, -4.93480213707883, 4.058709159556464, -1.335212003052184, 0.2349373138245546, -0.024396324364378108)


def poly(coeffs, z):
    total = coeffs[-1]
    for c in coeffs[-2::-1]:
        total = total * z + c
    return total


def dot(a, b, dims=((1,), (0,))):
    return lax.dot_general(a, b, (dims, ((), ())), preferred_element_type=F32)


def iota(shape, dim):
    return lax.broadcasted_iota(jnp.int32, shape, dim)


def exact(a, b, dims=((1,), (0,))):
    return lax.dot_general(a, b, (dims, ((), ())), precision=lax.Precision.HIGHEST, preferred_element_type=F32)


def cmul(ar, ai, br, bi):
    return ar * br - ai * bi, ar * bi + ai * br


def permutation(rows):
    run = rows // SUB
    r, t = iota((rows, rows), 0), iota((rows, rows), 1)
    return jnp.where((r % SUB) * run + r // SUB == t, 1.0, 0.0).astype(BF16)


def spread(mat, block, width, span, group, states):
    chans = slice(block * width, (block + 1) * width)
    tile = jnp.where(iota((states, span), 0) == iota((states, span), 1) % states, 1.0, 0.0).astype(BF16)
    keep = iota((width, span), 0) // group == iota((width, span), 1) // states
    return jnp.where(keep, dot(mat[chans, :], tile), 0.0).astype(BF16)


def couple(block, state_p, in_r, in_i, dr_ref, di_ref, group, states):
    width = state_p.shape[1]
    span = width // group * states
    cols = slice(block * span, (block + 1) * span)
    for src, dst in ((in_r, dr_ref), (in_i, di_ref)):
        dst[:, cols] = dot(state_p, spread(src, block, width, span, group, states))


def scan_block(lo, span, rate, coef, hr, hi, ar, ai):
    cols = pl.ds(lo, span)
    run = rate.shape[0] // SUB
    reps = span // 128
    decay = jnp.broadcast_to(coef[0:1, cols], (SUB, span))
    turn = jnp.broadcast_to(coef[1:2, cols], (SUB, span))

    def one(j, carry):
        h_r, h_i, a_r, a_i = carry
        at = pl.ds(pl.multiple_of(j * SUB, SUB), SUB)
        r = jnp.concatenate([rate[at, :]] * reps, axis=1)
        u = r * turn
        f = u - jnp.floor(u + 0.5)
        z = f * f
        s = f * poly(SIN, z)
        c = poly(COS, z)
        grow = jnp.exp(r * decay)
        gs = 2.0 * grow * s
        b_r = grow - gs * s
        b_i = gs * c
        p_r, p_i = cmul(b_r - 1.0, b_i, hr[at, cols], hi[at, cols])
        m_r, m_i = cmul(b_r, b_i, h_r, h_i)
        h_r, h_i = m_r + p_r, m_i + p_i
        a_r, a_i = cmul(b_r, b_i, a_r, a_i)
        hr[at, cols] = h_r
        hi[at, cols] = h_i
        ar[at, cols] = a_r
        ai[at, cols] = a_i
        return h_r, h_i, a_r, a_i

    zero = jnp.zeros((SUB, span), F32)
    lax.fori_loop(0, run, one, (zero, zero, zero + 1.0, zero), unroll=2)


def chain_subs(hr, hi, ar, ai, pre, summ):
    rows, flat = hr.shape
    last = rows - SUB
    m_r, m_i = jnp.ones((1, flat), F32), jnp.zeros((1, flat), F32)
    v_r, v_i = jnp.zeros((1, flat), F32), jnp.zeros((1, flat), F32)
    for s in range(SUB):
        row = slice(s, s + 1)
        pre[0, row, :], pre[1, row, :], pre[2, row, :], pre[3, row, :] = m_r, m_i, v_r, v_i
        at = slice(last + s, last + s + 1)
        e_r, e_i = ar[at, :], ai[at, :]
        m_r, m_i = cmul(e_r, e_i, m_r, m_i)
        w_r, w_i = cmul(e_r, e_i, v_r, v_i)
        v_r, v_i = w_r + hr[at, :], w_i + hi[at, :]
    summ[0:1, :], summ[1:2, :], summ[2:3, :], summ[3:4, :] = m_r, m_i, v_r, v_i


def enter_states(place, count, get, s_r, s_i):
    e_r, e_i = s_r, s_i
    for j in range(count):
        g = get(j)
        here = place == j
        e_r, e_i = jnp.where(here, s_r, e_r), jnp.where(here, s_i, e_i)
        t_r, t_i = cmul(g[0:1, :], g[1:2, :], s_r, s_i)
        s_r, s_i = t_r + g[2:3, :], t_i + g[3:4, :]
    return e_r, e_i, s_r, s_i


def compose(count, get):
    first = get(0)
    m_r, m_i, v_r, v_i = (first[k : k + 1, :] for k in range(4))
    for j in range(1, count):
        g = get(j)
        g_r, g_i = g[0:1, :], g[1:2, :]
        m_r, m_i = cmul(g_r, g_i, m_r, m_i)
        w_r, w_i = cmul(g_r, g_i, v_r, v_i)
        v_r, v_i = w_r + g[2:3, :], w_i + g[3:4, :]
    return m_r, m_i, v_r, v_i


def readout(block, width, state_p, enter, hr, hi, ar, ai, pre, rd_r, rd_i, skip, perm, out, group, states):
    span = width // group * states
    cols = slice(block * span, (block + 1) * span)
    chans = slice(block * width, (block + 1) * width)
    rows = hr.shape[0]
    run = rows // SUB
    e_r, e_i = cmul(pre[0, :, cols], pre[1, :, cols], enter[0][:, cols], enter[1][:, cols])
    e_r, e_i = e_r + pre[2, :, cols], e_i + pre[3, :, cols]
    g_r = spread(rd_r, block, width, span, group, states)
    g_i = spread(rd_i, block, width, span, group, states)

    def fixed(local, a, b, sign):
        a3, b3 = a[:, cols].reshape(run, SUB, span), b[:, cols].reshape(run, SUB, span)
        x, y = (e_r, e_i) if sign < 0 else (e_i, e_r)
        shift = a3 * x[None] + (b3 * y[None] if sign > 0 else -b3 * y[None])
        return (local[:, cols].reshape(run, SUB, span) + shift).reshape(rows, span).astype(BF16)

    total = dot(fixed(hr, ar, ai, -1), g_r, ((1,), (1,))) - dot(fixed(hi, ar, ai, 1), g_i, ((1,), (1,)))
    v = total + skip[:, chans] * state_p[:, chans].astype(F32)
    mix = 0.5 * v * (1.0 + jnp.tanh(0.7978845608 * (v + 0.044715 * (v * v * v))))
    out[:, chans] = dot(perm, mix.astype(BF16), ((0,), (0,))).astype(BF16)


def prepare_rates(step_rate, rate):
    rows = rate.shape[0]
    run = rows // SUB
    r, t = iota((rows, rows), 0), iota((rows, rows), 1)
    chosen = jnp.where((r % SUB) * run + r // SUB == t, jnp.broadcast_to(step_rate[...], (rows, rows)), 0.0)
    rate[...] = exact(chosen, jnp.ones((rows, 128), F32))


def flatten(parts, states):
    groups = parts[0].shape[0]
    flat = groups * states
    tile = jnp.where(iota((states, flat), 0) == iota((states, flat), 1) % states, 1.0, 0.0)
    keep = iota((groups, flat), 0) == iota((groups, flat), 1) // states
    return [jnp.sum(jnp.where(keep, exact(part, tile), 0.0), axis=0, keepdims=True) for part in parts]


def prepare_coefs(log_step, decay, frequency, initial, coef, opening):
    groups, states = decay.shape
    base = jnp.where(iota((groups, groups), 0) == iota((groups, groups), 1), jnp.broadcast_to(jnp.exp(log_step[...]), (groups, groups)), 0.0)
    base = jnp.sum(base, axis=1, keepdims=True)
    parts = [base * decay[...], base * frequency[...] * 0.15915494309189535, initial[0:groups, :], initial[groups:, :]]
    rows = flatten(parts, states)
    coef[0:1, :], coef[1:2, :], opening[0:1, :], opening[1:2, :] = rows


def prepare_inputs(decay, frequency, input_real, input_imag, in_r, in_i, group):
    groups = decay.shape[0]
    d, f = decay[...], frequency[...]
    modulus = d * d + f * f
    each = jnp.where(iota((groups * group, groups), 0) // group == iota((groups * group, groups), 1), 1.0, 0.0)
    inv_r, inv_i = exact(each, d / modulus), exact(each, -f / modulus)
    x_r, x_i = input_real[...], input_imag[...]
    in_r[...] = (x_r * inv_r - x_i * inv_i).astype(BF16)
    in_i[...] = (x_r * inv_i + x_i * inv_r).astype(BF16)


def prepare_skip(skip_gain, skip):
    group, groups = skip_gain.shape
    chans = groups * group
    each = jnp.where(iota((groups, chans), 0) == iota((groups, chans), 1) // group, 1.0, 0.0)
    keep = iota((group, chans), 0) == iota((group, chans), 1) % group
    skip[...] = jnp.sum(jnp.where(keep, exact(skip_gain[...], each), 0.0), axis=0, keepdims=True)


def own_states(row, sp, share, groups, states):
    flat = groups * states
    shape = (SUB, flat)
    mine = jnp.where(iota(shape, 1) % states == sp * share + iota(shape, 0), jnp.broadcast_to(row, shape), 0.0)
    each = jnp.where(iota((groups, flat), 0) == iota((groups, flat), 1) // states, 1.0, 0.0)
    return exact(mine, each, ((1,), (1,)))[0:share, :]


MESH = pl.DeviceIdType.MESH
HALO = 16
S, V, I, O, SO, CO = range(6)


def layer_kernel(sizes, *refs):
    n_sp, n_fs, n_tp, group, states = sizes
    inputs, (out, final), scratch = refs[:19], refs[19:21], refs[21:]
    hbm_weights, hbm_rest = inputs[:6], inputs[6:]
    local, scratch = scratch[:13], scratch[13:]
    (
        full, normed, state_p, hr, hi, ar, ai, pre, summ, near, total_map, far, fin_src, fin_dst, ext, halo_src, halo_dst,
        conv_mix, state_mix, partial, got, rate, coef, opening, in_r, in_i, rd_r, rd_i, skip,
        load, load_w, ring_send, ring_recv, sib_send, sib_recv, near_send, near_recv, far_send, far_recv, fin_send, fin_recv,
        x_send, x_recv, halo_send, halo_recv,
    ) = scratch
    tokens, gain, log_step, decay, frequency, step_rate, input_real, input_imag, read_real, read_imag, skip_gain, taps, initial = local
    shard = hbm_weights[0].shape[0]
    rows = tokens.shape[0]
    channels = hbm_weights[0].shape[1]
    sp, fs, tp = lax.axis_index("sp"), lax.axis_index("fs"), lax.axis_index("tp")
    pairs = n_sp * n_fs // 2
    half = pairs // 2
    inner = math.gcd(n_sp, 4)
    outer = n_sp // inner
    here, layer = sp % inner, sp // inner
    mine = sp * n_fs + fs
    parity, chip = mine % 2, mine // 2
    place = jnp.where(chip % 2 == 0, chip // 2, pairs - 1 - chip // 2)

    def own(w):
        return full.at[w, pl.ds(pl.multiple_of(mine * shard, shard), shard), :]

    loads = [pltpu.make_async_copy(src, own(w), load_w.at[w]) for w, src in enumerate(hbm_weights)]
    rest = [pltpu.make_async_copy(src, dst, load.at[k]) for k, (src, dst) in enumerate(zip(hbm_rest, local))]
    for copy in loads[:2] + rest[:1] + loads[2:] + rest[1:]:
        copy.start()

    def pair_at(offset):
        q = (place + offset + pairs) % pairs
        return jnp.where(q < half, q * 2, (pairs - 1 - q) * 2 + 1)

    def device(linear):
        return (linear // n_fs, linear % n_fs, tp)

    neighbours = (device(pair_at(1) * 2 + parity), device(pair_at(-1) * 2 + parity))
    sibling = device(chip * 2 + 1 - parity)
    near_peers = [(layer * inner + (here + s) % inner, fs, tp) for s in range(1, inner)]
    far_peers = [((sp + s * inner) % n_sp, fs, tp) for s in range(1, outer)]
    after, before = ((sp + 1) % n_sp, fs, tp), ((sp + n_sp - 1) % n_sp, fs, tp)
    tp_peers = [(sp, fs, (tp + s) % n_tp) for s in range(1, n_tp)]

    barrier = pltpu.get_barrier_semaphore()
    greet = list(neighbours) + [sibling] + near_peers + far_peers + tp_peers + [after, before]
    for other in greet:
        pl.semaphore_signal(barrier, inc=1, device_id=other, device_id_type=MESH)
    pl.semaphore_wait(barrier, len(greet))

    sent = []

    def remote(src, dst, s_sem, r_sem, to):
        return pltpu.make_async_remote_copy(src_ref=src, dst_ref=dst, send_sem=s_sem, recv_sem=r_sem, device_id=to, device_id_type=MESH)

    def send(src, dst, s_sem, r_sem, to):
        copy = remote(src, dst, s_sem, r_sem, to)
        copy.start()
        sent.append(copy)

    def landed(ref, s_sem, r_sem):
        pltpu.make_async_remote_copy(
            src_ref=ref, dst_ref=ref, send_sem=s_sem, recv_sem=r_sem, device_id=sibling, device_id_type=MESH
        ).wait_recv()

    def slot(w, pair, par):
        return full.at[w, pl.ds(pl.multiple_of((pair * 2 + par) * shard, shard), shard), :]

    def rounds(w, way):
        return half if way == w % 2 else pairs - 1 - half

    def source(way, r):
        return pair_at(-1 - r if way == 0 else 1 + r)

    arrived = set()
    shared = set()

    def arrive(w, way, r):
        if (w, way, r) in arrived:
            return
        arrived.add((w, way, r))
        ref = slot(w, source(way, r), parity)
        landed(ref, ring_send.at[w, way, r], ring_recv.at[w, way, r])
        d = 1 + way * half + r
        send(ref, ref, sib_send.at[w, d], sib_recv.at[w, d], sibling)

    def share(w, d, pair):
        if (w, d) not in shared:
            shared.add((w, d))
            landed(slot(w, pair, 1 - parity), sib_send.at[w, d], sib_recv.at[w, d])

    def issue(w, r):
        if r == 0:
            loads[w].wait()
        for way in range(2):
            if r >= rounds(w, way):
                continue
            if r == 0:
                src, at = own(w), chip
            else:
                arrive(w, way, r - 1)
                at = source(way, r - 1)
                src = slot(w, at, parity)
            send(src, slot(w, at, parity), ring_send.at[w, way, r], ring_recv.at[w, way, r], neighbours[way])
        if r == 0:
            send(own(w), own(w), sib_send.at[w, 0], sib_recv.at[w, 0], sibling)

    queue = []
    fresh = {w: 0 for w in range(6)}

    def plan(*ws):
        for w in ws:
            if fresh[w] < half:
                queue.append((w, fresh[w]))
                fresh[w] += 1
                if fresh[w] == half:
                    queue.append((w, half))

    plan(S, V, I)
    for r in range(1, half):
        plan(S, V)
    plan(O, I, SO)
    for r in range(1, half):
        plan(O, I)
    plan(CO)
    for r in range(1, half):
        plan(SO, CO)
    done = [0]

    def advance(count):
        for w, r in queue[done[0] : done[0] + count]:
            done[0] += 1
            if r < half:
                issue(w, r)
            else:
                for way in range(2):
                    for k in range(rounds(w, way)):
                        arrive(w, way, k)

    def until(w, r):
        advance(queue.index((w, r)) + 1 - done[0])

    def finish(w):
        until(w, half)
        share(w, 0, chip)
        for r in range(half):
            for way in range(2):
                if r < rounds(w, way):
                    share(w, 1 + way * half + r, source(way, r))

    advance(3)
    rest[0].wait()
    rest[1].wait()

    def norm(j, carry):
        at = pl.ds(pl.multiple_of(j * 32, 32), 32)
        x = tokens[at, :].astype(F32)
        scale = lax.rsqrt(jnp.mean(x * x, axis=-1, keepdims=True) + 1e-06)
        normed[at, :] = (x * scale * gain[...]).astype(BF16)
        return carry

    lax.fori_loop(0, rows // 32, norm, 0)
    for copy in rest[2:]:
        copy.wait()
    advance(1)
    perm = permutation(rows)
    prepare_rates(step_rate, rate)
    advance(1)
    prepare_coefs(log_step, decay, frequency, initial, coef, opening)
    advance(1)
    prepare_inputs(decay, frequency, input_real, input_imag, in_r, in_i, group)
    rd_r[...] = read_real[...].astype(BF16)
    rd_i[...] = read_imag[...].astype(BF16)
    prepare_skip(skip_gain, skip)
    finish(S)

    def project(w):
        return dot(normed[...], full[w]).astype(BF16)

    state_p[...] = dot(perm, project(S)).astype(BF16)
    width = min(128, channels)
    span = width // group * states
    blocks = channels // width
    for block in range(blocks):
        couple(block, state_p[:, block * width : (block + 1) * width], in_r, in_i, hr, hi, group, states)
        scan_block(block * span, span, rate, coef, hr, hi, ar, ai)
        advance(1)
    chain_subs(hr, hi, ar, ai, pre, summ)
    for s, other in enumerate(near_peers):
        send(summ, near.at[here], near_send.at[s], near_recv.at[s], other)
    near[pl.ds(here, 1)] = summ[...][None]
    finish(V)
    value = project(V)
    advance(1)
    for s in range(1, inner):
        landed(near.at[(here + inner - s) % inner], near_send.at[s - 1], near_recv.at[s - 1])
    for k, row in enumerate(compose(inner, lambda j: near[j])):
        total_map[k : k + 1, :] = row
    far[pl.ds(layer, 1)] = total_map[...][None]
    for s, other in enumerate(far_peers, 1):

        @pl.when(layer + s < outer)
        def _():
            remote(total_map, far.at[layer], far_send.at[s - 1], far_recv.at[s - 1], other).start()

    advance(1)
    for s in range(1, outer):

        @pl.when(layer >= s)
        def _():
            landed(far.at[layer - s], far_send.at[s - 1], far_recv.at[s - 1])

    l_r, l_i, s_r, s_i = enter_states(layer, outer, lambda j: far[j], opening[0:1, :], opening[1:2, :])
    e_r, e_i, _, _ = enter_states(here, inner, lambda j: near[j], l_r, l_i)
    fin_src[0:1, :] = s_r
    fin_src[1:2, :] = s_i
    last = layer == outer - 1
    for s in range(1, outer):

        @pl.when(last)
        def _():
            remote(fin_src, fin_dst, fin_send.at[s - 1], fin_recv, far_peers[outer - 1 - s]).start()

    advance(1)
    for block in range(blocks):
        readout(block, width, state_p, (e_r, e_i), hr, hi, ar, ai, pre, rd_r, rd_i, skip, perm, state_mix, group, states)
        advance(1)
    finish(I)
    product = (project(I).astype(F32) * value.astype(F32)).astype(BF16)
    halo_src[...] = product[rows - HALO :, :]
    ext[HALO:, :] = product.astype(F32)
    send(halo_src, halo_dst, halo_send, halo_recv, after)
    finish(O)
    outward = project(O)
    advance(1)
    landed(halo_dst, halo_send, halo_recv)
    ext[:HALO, :] = jnp.where(sp == 0, 0.0, halo_dst[...].astype(F32))
    reach = taps.shape[0] - 1
    filtered = taps[0:1, :] * ext[HALO - reach : HALO - reach + rows, :]
    for tap in range(1, reach + 1):
        at = HALO - reach + tap
        filtered = filtered + taps[tap : tap + 1, :] * ext[at : at + rows, :]
    conv_mix[...] = (outward.astype(F32) * filtered).astype(BF16)
    advance(1)
    own_rows = rows // n_tp
    chunks = []

    def compute(pair):
        c = len(chunks)
        at = pl.ds(pl.multiple_of(pair * 2 * shard, 2 * shard), 2 * shard)
        partial[pl.ds(pair, 1)] = (
            dot(state_mix[...], full[SO, at, :], ((1,), (1,))) + dot(conv_mix[...], full[CO, at, :], ((1,), (1,)))
        ).astype(BF16)[None]
        chunks.append(pair)
        if c > 0:
            exchange(c - 1)

    def exchange(c):
        pair = chunks[c]
        for s, other in enumerate(tp_peers):
            theirs = pl.ds(pl.multiple_of(other[2] * own_rows, own_rows), own_rows)
            send(partial.at[pair, theirs, :], got.at[pair, s], x_send.at[c, s], x_recv.at[c, s], other)

    share(SO, 0, chip)
    share(CO, 0, chip)
    compute(chip)
    for r in range(half):
        for w in (SO, CO):
            until(w, r + 1)
        for way in range(2):
            for w in (SO, CO):
                if r < rounds(w, way):
                    arrive(w, way, r)
        ways = (0, 1)
        for way in ways if r < half - 1 else ways[:1]:
            for each in (way,) if r < half - 1 else ways:
                for w in (SO, CO):
                    if r < rounds(w, each):
                        share(w, 1 + each * half + r, source(each, r))
            compute(source(way, r))
    exchange(len(chunks) - 1)

    @pl.when(jnp.logical_not(last))
    def _():
        landed(fin_dst, fin_send.at[0], fin_recv)

    share_states = states // n_sp
    groups = decay.shape[0]
    for k in range(2):
        row = jnp.where(last, fin_src[k : k + 1, :], fin_dst[k : k + 1, :])
        final[k] = own_states(row, sp, share_states, groups, states)
    kept = pl.ds(pl.multiple_of(tp * own_rows, own_rows), own_rows)
    for c, pair in enumerate(chunks):
        for s in range(n_tp - 1):
            landed(got.at[pair, s], x_send.at[c, s], x_recv.at[c, s])
    for k in range(pairs):
        total = partial[k, kept, :].astype(F32)
        for s in range(n_tp - 1):
            total = total + got[k, s].astype(F32)
        out[:, k * 2 * shard : (k + 1) * 2 * shard] = total.astype(BF16)
    for copy in sent:
        copy.wait_send()
    for s, other in enumerate(far_peers, 1):

        @pl.when(layer + s < outer)
        def _():
            remote(total_map, far.at[layer], far_send.at[s - 1], far_recv.at[s - 1], other).wait_send()

        @pl.when(last)
        def _():
            remote(fin_src, fin_dst, fin_send.at[s - 1], fin_recv, other).wait_send()


def body(tokens, norm_gain, w_state_in, w_value, w_outer, w_inner, w_state_out, w_conv_out, log_step, decay_real, frequency, step_rate, input_real, input_imag, read_real, read_imag, skip_gain, conv_taps, initial_state):
    rows, features = tokens.shape[1:]
    groups, states = decay_real.shape
    group = skip_gain.shape[1]
    flat = groups * states
    channels = groups * group
    conv = conv_taps.shape[1]
    n_sp, n_fs, n_tp = (lax.axis_size(a) for a in ("sp", "fs", "tp"))
    shard = w_state_in.shape[0]
    pairs = n_sp * n_fs // 2
    half = pairs // 2
    inner = math.gcd(n_sp, 4)
    outer = n_sp // inner
    share = states // n_sp
    rest = (
        tokens[0], norm_gain[None], log_step[None], decay_real, frequency, step_rate,
        jnp.swapaxes(input_real, 1, 2).reshape(channels, states), jnp.swapaxes(input_imag, 1, 2).reshape(channels, states),
        read_real.reshape(channels, states), read_imag.reshape(channels, states), skip_gain.T, conv_taps,
        initial_state.reshape(2 * groups, states),
    )
    vmem = pltpu.VMEM
    dma = pltpu.SemaphoreType.DMA
    out, final = pl.pallas_call(
        lambda *refs: layer_kernel((n_sp, n_fs, n_tp, group, states), *refs),
        out_shape=(jax.ShapeDtypeStruct((rows // n_tp, features), BF16), jax.ShapeDtypeStruct((2, share, groups), F32)),
        in_specs=[pl.BlockSpec(memory_space=pl.ANY)] * 19,
        out_specs=[pl.BlockSpec(memory_space=vmem)] * 2,
        scratch_shapes=[
            *[vmem(a.shape, a.dtype) for a in rest],
            vmem((6, n_sp * n_fs * shard, channels), BF16),
            vmem((rows, features), BF16),
            vmem((rows, channels), BF16),
            *[vmem((rows, flat), F32)] * 4,
            vmem((4, SUB, flat), F32),
            vmem((4, flat), F32),
            vmem((inner, 4, flat), F32),
            vmem((4, flat), F32),
            vmem((outer, 4, flat), F32),
            vmem((2, flat), F32),
            vmem((2, flat), F32),
            vmem((rows + HALO, conv), F32),
            vmem((HALO, conv), BF16),
            vmem((HALO, conv), BF16),
            vmem((rows, conv), BF16),
            vmem((rows, channels), BF16),
            vmem((pairs, rows, 2 * shard), BF16),
            vmem((pairs, n_tp - 1, rows // n_tp, 2 * shard), BF16),
            vmem((rows, 128), F32),
            vmem((2, flat), F32),
            vmem((2, flat), F32),
            *[vmem((channels, states), BF16)] * 4,
            vmem((1, channels), F32),
            dma((13,)),
            dma((6,)),
            dma((6, 2, half)),
            dma((6, 2, half)),
            dma((6, 1 + 2 * half)),
            dma((6, 1 + 2 * half)),
            dma((inner - 1,)),
            dma((inner - 1,)),
            dma((outer - 1,)),
            dma((outer - 1,)),
            dma((outer - 1,)),
            dma,
            dma((pairs, n_tp - 1)),
            dma((pairs, n_tp - 1)),
            dma,
            dma,
        ],
        compiler_params=pltpu.CompilerParams(collective_id=0, has_side_effects=True, vmem_limit_bytes=60000 * 1024),
        name="layer",
    )(w_state_in, w_value, w_inner, w_outer, w_state_out, w_conv_out, *rest)
    return out[None], jnp.swapaxes(final, 1, 2)[None]


def solution(mesh):
    return jax.shard_map(
        body,
        mesh=mesh,
        in_specs=(
            P("fs", "sp", None),
            P(),
            P(("sp", "fs"), "tp"),
            P(("sp", "fs"), "tp"),
            P(("sp", "fs"), "tp"),
            P(("sp", "fs"), "tp"),
            P(("sp", "fs"), "tp"),
            P(("sp", "fs"), "tp"),
            P("tp"),
            P("tp", None),
            P("tp", None),
            P("fs", "sp"),
            P("tp", None, None),
            P("tp", None, None),
            P("tp", None, None),
            P("tp", None, None),
            P("tp", None),
            P(None, "tp"),
            P("fs", None, "tp", None),
        ),
        out_specs=(P("fs", ("sp", "tp"), None), P("fs", None, "tp", "sp")),
        check_vma=False,
    )
```

```python
import math

import jax
import jax.numpy as jnp
from jax import lax
from jax.experimental import pallas as pl
from jax.experimental.pallas import tpu as pltpu
from jax.sharding import PartitionSpec as P

F32 = jnp.float32
BF16 = jnp.bfloat16
SUB = 8
SIN = (3.1415925798055846, -5.16770686616794, 2.5500311935192803, -0.5980441939118888, 0.07721838615680923)
COS = (0.9999999997799038, -4.93480213707883, 4.058709159556464, -1.335212003052184, 0.2349373138245546, -0.024396324364378108)


def poly(coeffs, z):
    total = coeffs[-1]
    for c in coeffs[-2::-1]:
        total = total * z + c
    return total


def dot(a, b, dims=((1,), (0,))):
    return lax.dot_general(a, b, (dims, ((), ())), preferred_element_type=F32)


def iota(shape, dim):
    return lax.broadcasted_iota(jnp.int32, shape, dim)


def exact(a, b, dims=((1,), (0,))):
    return lax.dot_general(a, b, (dims, ((), ())), precision=lax.Precision.HIGHEST, preferred_element_type=F32)


def cmul(ar, ai, br, bi):
    return ar * br - ai * bi, ar * bi + ai * br


def permutation(rows):
    run = rows // SUB
    r, t = iota((rows, rows), 0), iota((rows, rows), 1)
    return jnp.where((r % SUB) * run + r // SUB == t, 1.0, 0.0).astype(BF16)


def spread(mat, block, width, span, group, states):
    chans = slice(block * width, (block + 1) * width)
    tile = jnp.where(iota((states, span), 0) == iota((states, span), 1) % states, 1.0, 0.0).astype(BF16)
    keep = iota((width, span), 0) // group == iota((width, span), 1) // states
    return jnp.where(keep, dot(mat[chans, :], tile), 0.0).astype(BF16)


def couple(block, state_p, in_r, in_i, dr_ref, di_ref, group, states):
    width = state_p.shape[1]
    span = width // group * states
    cols = slice(block * span, (block + 1) * span)
    for src, dst in ((in_r, dr_ref), (in_i, di_ref)):
        dst[:, cols] = dot(state_p, spread(src, block, width, span, group, states))


def scan_block(lo, span, rate, coef, hr, hi, ar, ai):
    cols = pl.ds(lo, span)
    run = rate.shape[0] // SUB
    reps = span // 128
    decay = jnp.broadcast_to(coef[0:1, cols], (SUB, span))
    turn = jnp.broadcast_to(coef[1:2, cols], (SUB, span))

    def one(j, carry):
        h_r, h_i, a_r, a_i = carry
        at = pl.ds(pl.multiple_of(j * SUB, SUB), SUB)
        r = jnp.concatenate([rate[at, :]] * reps, axis=1)
        u = r * turn
        f = u - jnp.floor(u + 0.5)
        z = f * f
        s = f * poly(SIN, z)
        c = poly(COS, z)
        grow = jnp.exp(r * decay)
        gs = 2.0 * grow * s
        b_r = grow - gs * s
        b_i = gs * c
        p_r, p_i = cmul(b_r - 1.0, b_i, hr[at, cols], hi[at, cols])
        m_r, m_i = cmul(b_r, b_i, h_r, h_i)
        h_r, h_i = m_r + p_r, m_i + p_i
        a_r, a_i = cmul(b_r, b_i, a_r, a_i)
        hr[at, cols] = h_r
        hi[at, cols] = h_i
        ar[at, cols] = a_r
        ai[at, cols] = a_i
        return h_r, h_i, a_r, a_i

    zero = jnp.zeros((SUB, span), F32)
    lax.fori_loop(0, run, one, (zero, zero, zero + 1.0, zero), unroll=2)


def chain_subs(hr, hi, ar, ai, pre, summ):
    rows, flat = hr.shape
    last = rows - SUB
    m_r, m_i = jnp.ones((1, flat), F32), jnp.zeros((1, flat), F32)
    v_r, v_i = jnp.zeros((1, flat), F32), jnp.zeros((1, flat), F32)
    for s in range(SUB):
        row = slice(s, s + 1)
        pre[0, row, :], pre[1, row, :], pre[2, row, :], pre[3, row, :] = m_r, m_i, v_r, v_i
        at = slice(last + s, last + s + 1)
        e_r, e_i = ar[at, :], ai[at, :]
        m_r, m_i = cmul(e_r, e_i, m_r, m_i)
        w_r, w_i = cmul(e_r, e_i, v_r, v_i)
        v_r, v_i = w_r + hr[at, :], w_i + hi[at, :]
    summ[0:1, :], summ[1:2, :], summ[2:3, :], summ[3:4, :] = m_r, m_i, v_r, v_i


def enter_states(place, count, get, s_r, s_i):
    e_r, e_i = s_r, s_i
    for j in range(count):
        g = get(j)
        here = place == j
        e_r, e_i = jnp.where(here, s_r, e_r), jnp.where(here, s_i, e_i)
        t_r, t_i = cmul(g[0:1, :], g[1:2, :], s_r, s_i)
        s_r, s_i = t_r + g[2:3, :], t_i + g[3:4, :]
    return e_r, e_i, s_r, s_i


def compose(count, get):
    first = get(0)
    m_r, m_i, v_r, v_i = (first[k : k + 1, :] for k in range(4))
    for j in range(1, count):
        g = get(j)
        g_r, g_i = g[0:1, :], g[1:2, :]
        m_r, m_i = cmul(g_r, g_i, m_r, m_i)
        w_r, w_i = cmul(g_r, g_i, v_r, v_i)
        v_r, v_i = w_r + g[2:3, :], w_i + g[3:4, :]
    return m_r, m_i, v_r, v_i


def readout(block, width, state_p, enter, hr, hi, ar, ai, pre, rd_r, rd_i, skip, perm, out, group, states):
    span = width // group * states
    cols = slice(block * span, (block + 1) * span)
    chans = slice(block * width, (block + 1) * width)
    rows = hr.shape[0]
    run = rows // SUB
    e_r, e_i = cmul(pre[0, :, cols], pre[1, :, cols], enter[0][:, cols], enter[1][:, cols])
    e_r, e_i = e_r + pre[2, :, cols], e_i + pre[3, :, cols]
    g_r = spread(rd_r, block, width, span, group, states)
    g_i = spread(rd_i, block, width, span, group, states)

    def fixed(local, a, b, sign):
        a3, b3 = a[:, cols].reshape(run, SUB, span), b[:, cols].reshape(run, SUB, span)
        x, y = (e_r, e_i) if sign < 0 else (e_i, e_r)
        shift = a3 * x[None] + (b3 * y[None] if sign > 0 else -b3 * y[None])
        return (local[:, cols].reshape(run, SUB, span) + shift).reshape(rows, span).astype(BF16)

    total = dot(fixed(hr, ar, ai, -1), g_r, ((1,), (1,))) - dot(fixed(hi, ar, ai, 1), g_i, ((1,), (1,)))
    v = total + skip[:, chans] * state_p[:, chans].astype(F32)
    mix = 0.5 * v * (1.0 + jnp.tanh(0.7978845608 * (v + 0.044715 * (v * v * v))))
    out[:, chans] = dot(perm, mix.astype(BF16), ((0,), (0,))).astype(BF16)


def prepare_rates(step_rate, rate):
    rows = rate.shape[0]
    run = rows // SUB
    r, t = iota((rows, rows), 0), iota((rows, rows), 1)
    chosen = jnp.where((r % SUB) * run + r // SUB == t, jnp.broadcast_to(step_rate[...], (rows, rows)), 0.0)
    rate[...] = exact(chosen, jnp.ones((rows, 128), F32))


def flatten(parts, states):
    groups = parts[0].shape[0]
    flat = groups * states
    tile = jnp.where(iota((states, flat), 0) == iota((states, flat), 1) % states, 1.0, 0.0)
    keep = iota((groups, flat), 0) == iota((groups, flat), 1) // states
    return [jnp.sum(jnp.where(keep, exact(part, tile), 0.0), axis=0, keepdims=True) for part in parts]


def prepare_coefs(log_step, decay, frequency, initial, coef, opening):
    groups, states = decay.shape
    base = jnp.where(iota((groups, groups), 0) == iota((groups, groups), 1), jnp.broadcast_to(jnp.exp(log_step[...]), (groups, groups)), 0.0)
    base = jnp.sum(base, axis=1, keepdims=True)
    parts = [base * decay[...], base * frequency[...] * 0.15915494309189535, initial[0:groups, :], initial[groups:, :]]
    rows = flatten(parts, states)
    coef[0:1, :], coef[1:2, :], opening[0:1, :], opening[1:2, :] = rows


def prepare_inputs(decay, frequency, input_real, input_imag, in_r, in_i, group):
    groups = decay.shape[0]
    d, f = decay[...], frequency[...]
    modulus = d * d + f * f
    each = jnp.where(iota((groups * group, groups), 0) // group == iota((groups * group, groups), 1), 1.0, 0.0)
    inv_r, inv_i = exact(each, d / modulus), exact(each, -f / modulus)
    x_r, x_i = input_real[...], input_imag[...]
    in_r[...] = (x_r * inv_r - x_i * inv_i).astype(BF16)
    in_i[...] = (x_r * inv_i + x_i * inv_r).astype(BF16)


def prepare_skip(skip_gain, skip):
    group, groups = skip_gain.shape
    chans = groups * group
    each = jnp.where(iota((groups, chans), 0) == iota((groups, chans), 1) // group, 1.0, 0.0)
    keep = iota((group, chans), 0) == iota((group, chans), 1) % group
    skip[...] = jnp.sum(jnp.where(keep, exact(skip_gain[...], each), 0.0), axis=0, keepdims=True)


def own_states(row, sp, share, groups, states):
    flat = groups * states
    shape = (SUB, flat)
    mine = jnp.where(iota(shape, 1) % states == sp * share + iota(shape, 0), jnp.broadcast_to(row, shape), 0.0)
    each = jnp.where(iota((groups, flat), 0) == iota((groups, flat), 1) // states, 1.0, 0.0)
    return exact(mine, each, ((1,), (1,)))[0:share, :]


MESH = pl.DeviceIdType.MESH
HALO = 16
AHEAD = 5


def pieces_of(shard):
    return 2 if shard >= 64 else 1


S, V, I, O, SO, CO = range(6)


def layer_kernel(sizes, *refs):
    n_sp, n_fs, n_tp, group, states = sizes
    inputs, (out, final), scratch = refs[:19], refs[19:21], refs[21:]
    hbm_weights, hbm_rest = inputs[:6], inputs[6:]
    local, scratch = scratch[:13], scratch[13:]
    (
        full, normed, state_p, hr, hi, ar, ai, pre, summ, near, total_map, far, fin_src, fin_dst, ext, halo_src, halo_dst,
        conv_mix, state_mix, partial, got, rate, coef, opening, in_r, in_i, rd_r, rd_i, skip,
        load, load_w, ring_send, ring_recv, sib_send, sib_recv, near_send, near_recv, far_send, far_recv, fin_send, fin_recv,
        x_send, x_recv, halo_send, halo_recv,
    ) = scratch
    tokens, gain, log_step, decay, frequency, step_rate, input_real, input_imag, read_real, read_imag, skip_gain, taps, initial = local
    shard = hbm_weights[0].shape[0]
    rows = tokens.shape[0]
    channels = hbm_weights[0].shape[1]
    sp, fs, tp = lax.axis_index("sp"), lax.axis_index("fs"), lax.axis_index("tp")
    pairs = n_sp * n_fs // 2
    half = pairs // 2
    parts = pieces_of(shard)
    piece = shard // parts
    inner = math.gcd(n_sp, 4)
    outer = n_sp // inner
    here, layer = sp % inner, sp // inner
    mine = sp * n_fs + fs
    parity, chip = mine % 2, mine // 2
    place = jnp.where(chip % 2 == 0, chip // 2, pairs - 1 - chip // 2)

    def own(w):
        return full.at[w, pl.ds(pl.multiple_of(mine * shard, shard), shard), :]

    loads = [pltpu.make_async_copy(src, own(w), load_w.at[w]) for w, src in enumerate(hbm_weights)]
    rest = [pltpu.make_async_copy(src, dst, load.at[k]) for k, (src, dst) in enumerate(zip(hbm_rest, local))]
    for copy in loads[:2] + rest[:1] + loads[2:] + rest[1:]:
        copy.start()

    def pair_at(offset):
        q = (place + offset + pairs) % pairs
        return jnp.where(q < half, q * 2, (pairs - 1 - q) * 2 + 1)

    def device(linear):
        return (linear // n_fs, linear % n_fs, tp)

    neighbours = (device(pair_at(1) * 2 + parity), device(pair_at(-1) * 2 + parity))
    sibling = device(chip * 2 + 1 - parity)
    near_peers = [(layer * inner + (here + s) % inner, fs, tp) for s in range(1, inner)]
    far_peers = [((sp + s * inner) % n_sp, fs, tp) for s in range(1, outer)]
    after, before = ((sp + 1) % n_sp, fs, tp), ((sp + n_sp - 1) % n_sp, fs, tp)
    tp_peers = [(sp, fs, (tp + s) % n_tp) for s in range(1, n_tp)]

    barrier = pltpu.get_barrier_semaphore()
    greet = list(neighbours) + [sibling] + near_peers + far_peers + tp_peers + [after, before]
    for other in greet:
        pl.semaphore_signal(barrier, inc=1, device_id=other, device_id_type=MESH)
    pl.semaphore_wait(barrier, len(greet))

    def remote(src, dst, s_sem, r_sem, to):
        return pltpu.make_async_remote_copy(src_ref=src, dst_ref=dst, send_sem=s_sem, recv_sem=r_sem, device_id=to, device_id_type=MESH)

    def send(src, dst, s_sem, r_sem, to):
        remote(src, dst, s_sem, r_sem, to).start()

    def landed(ref, r_sem):
        remote(ref, ref, r_sem, r_sem, sibling).wait_recv()

    def gone(ref, s_sem):
        remote(ref, ref, s_sem, s_sem, sibling).wait_send()

    def slot(w, pair, par, h):
        return full.at[w, pl.ds(pl.multiple_of((pair * 2 + par) * shard + h * piece, piece), piece), :]

    def rounds(w, way):
        return half if way == w % 2 else pairs - 1 - half

    def source(way, r):
        return pair_at(-1 - r if way == 0 else 1 + r)

    def ways(w, r):
        return [way for way in range(2) if r < rounds(w, way)]

    def rows_of(w, count):
        return full.at[w, pl.ds(0, count), :]

    def sib_sem(w, r):
        return sib_recv.at[w if w < SO else SO + 1 + r]

    def share(r):
        count = 2 if r < 0 else sum(len(ways(w, r)) for w in (SO, CO))
        landed(rows_of(SO, count * shard), sib_sem(SO, r))

    last_round = half - 1
    units = [(S, 0), (V, 0)]
    for r in range(1, last_round):
        units += [(S, r), (V, r)]
    units += [(I, 0), (S, last_round), (V, last_round), (O, 0)]
    outputs = [(w, r) for r in range(last_round + 1) for w in (SO, CO)]
    for r in range(1, last_round + 1):
        units += [(I, r), outputs.pop(0), (O, r)]
    units += outputs
    pieces = [(w, r, h) for w, r in units for h in range(parts)]
    where = {item: k for k, item in enumerate(pieces)}
    sent_to, seen = [0], [0]

    def send_piece(w, r, h):
        if r == 0 and h == 0:
            loads[w].wait()
        for way in ways(w, r):
            at = chip if r == 0 else source(way, r - 1)
            ref = slot(w, at, parity, h)
            send(ref, ref, ring_send.at[w], ring_recv.at[w, r, h], neighbours[way])
        if r == 0 and h == parts - 1:
            send(own(w), own(w), sib_send.at[w], sib_sem(w, -1), sibling)

    def feed():
        while sent_to[0] < len(pieces) and sent_to[0] <= seen[0] + AHEAD:
            w, r, h = pieces[sent_to[0]]
            if r > 0 and where[w, r - 1, h] >= seen[0]:
                break
            send_piece(w, r, h)
            sent_to[0] += 1

    def pump(count=1):
        for _ in range(count):
            if seen[0] == len(pieces):
                return
            w, r, h = pieces[seen[0]]
            landed(rows_of(w, len(ways(w, r)) * piece), ring_recv.at[w, r, h])
            seen[0] += 1
            feed()
            for way in ways(w, r):
                ref = slot(w, source(way, r), parity, h)
                send(ref, ref, sib_send.at[w], sib_sem(w, r), sibling)

    def until(w, r):
        pump(max(0, where[w, r, parts - 1] + 1 - seen[0]))

    def finish(w):
        until(w, last_round)
        landed(rows_of(w, pairs * shard), sib_sem(w, 0))

    feed()
    rest[0].wait()
    rest[1].wait()

    def norm(j, carry):
        at = pl.ds(pl.multiple_of(j * 32, 32), 32)
        x = tokens[at, :].astype(F32)
        scale = lax.rsqrt(jnp.mean(x * x, axis=-1, keepdims=True) + 1e-06)
        normed[at, :] = (x * scale * gain[...]).astype(BF16)
        return carry

    lax.fori_loop(0, rows // 32, norm, 0)
    for copy in rest[2:]:
        copy.wait()
    pump()
    perm = permutation(rows)
    prepare_rates(step_rate, rate)
    pump()
    prepare_coefs(log_step, decay, frequency, initial, coef, opening)
    pump()
    prepare_inputs(decay, frequency, input_real, input_imag, in_r, in_i, group)
    pump()
    rd_r[...] = read_real[...].astype(BF16)
    rd_i[...] = read_imag[...].astype(BF16)
    prepare_skip(skip_gain, skip)
    finish(S)

    def project(w):
        return dot(normed[...], full[w]).astype(BF16)

    state_p[...] = dot(perm, project(S)).astype(BF16)
    pump(2)
    width = min(128, channels)
    span = width // group * states
    blocks = channels // width
    for block in range(blocks):
        couple(block, state_p[:, block * width : (block + 1) * width], in_r, in_i, hr, hi, group, states)
        scan_block(block * span, span, rate, coef, hr, hi, ar, ai)
        pump()
    chain_subs(hr, hi, ar, ai, pre, summ)
    for other in near_peers:
        send(summ, near.at[here], near_send, near_recv, other)
    near[pl.ds(here, 1)] = summ[...][None]
    finish(V)
    value = project(V)
    pump(4)
    landed(near.at[pl.ds(0, inner - 1)], near_recv)
    for k, row in enumerate(compose(inner, lambda j: near[j])):
        total_map[k : k + 1, :] = row
    far[pl.ds(layer, 1)] = total_map[...][None]
    for s, other in enumerate(far_peers, 1):

        @pl.when(layer + s < outer)
        def _():
            remote(total_map, far.at[layer], far_send.at[s - 1], far_recv.at[s - 1], other).start()

    finish(I)
    product = (project(I).astype(F32) * value.astype(F32)).astype(BF16)
    halo_src[...] = product[rows - HALO :, :]
    ext[HALO:, :] = product.astype(F32)
    pump()
    send(halo_src, halo_dst, halo_send, halo_recv, after)
    for s in range(1, outer):

        @pl.when(layer >= s)
        def _():
            landed(far.at[layer - s], far_recv.at[s - 1])

    l_r, l_i, s_r, s_i = enter_states(layer, outer, lambda j: far[j], opening[0:1, :], opening[1:2, :])
    e_r, e_i, _, _ = enter_states(here, inner, lambda j: near[j], l_r, l_i)
    fin_src[0:1, :] = s_r
    fin_src[1:2, :] = s_i
    last = layer == outer - 1
    for block in range(blocks):
        readout(block, width, state_p, (e_r, e_i), hr, hi, ar, ai, pre, rd_r, rd_i, skip, perm, state_mix, group, states)
        if block % 2 == 1:
            pump()
    for s in range(1, outer):

        @pl.when(last)
        def _():
            remote(fin_src, fin_dst, fin_send.at[s - 1], fin_recv, far_peers[outer - 1 - s]).start()

    finish(O)
    outward = project(O)
    landed(halo_dst, halo_recv)
    ext[:HALO, :] = jnp.where(sp == 0, 0.0, halo_dst[...].astype(F32))
    reach = taps.shape[0] - 1
    filtered = taps[0:1, :] * ext[HALO - reach : HALO - reach + rows, :]
    for tap in range(1, reach + 1):
        at = HALO - reach + tap
        filtered = filtered + taps[tap : tap + 1, :] * ext[at : at + rows, :]
    conv_mix[...] = (outward.astype(F32) * filtered).astype(BF16)
    pump()
    own_rows = rows // n_tp
    chunks = []

    def compute(pair):
        at = pl.ds(pl.multiple_of(pair * 2 * shard, 2 * shard), 2 * shard)
        partial[pl.ds(pair, 1)] = (
            dot(state_mix[...], full[SO, at, :], ((1,), (1,))) + dot(conv_mix[...], full[CO, at, :], ((1,), (1,)))
        ).astype(BF16)[None]

    def exchange(pair):
        for s, other in enumerate(tp_peers):
            theirs = pl.ds(pl.multiple_of(other[2] * own_rows, own_rows), own_rows)
            send(partial.at[pair, theirs, :], got.at[pair, s], x_send, x_recv.at[len(chunks)], other)
        chunks.append(pair)

    until(CO, 0)
    share(-1)
    compute(chip)
    exchange(chip)
    for r in range(half):
        until(SO, r)
        until(CO, r)
        share(r)
        fresh = [source(way, r) for way in ways(SO, r) if r < last_round or way == 0]
        for pair in fresh:
            compute(pair)
        for pair in fresh:
            exchange(pair)
        pump()

    @pl.when(jnp.logical_not(last))
    def _():
        landed(fin_dst, fin_recv)

    share_states = states // n_sp
    groups = decay.shape[0]
    for k in range(2):
        row = jnp.where(last, fin_src[k : k + 1, :], fin_dst[k : k + 1, :])
        final[k] = own_states(row, sp, share_states, groups, states)
    kept = pl.ds(pl.multiple_of(tp * own_rows, own_rows), own_rows)
    def settle(k, cols):
        total = partial[k, kept, :].astype(F32)
        for s in range(n_tp - 1):
            total = total + got[k, s].astype(F32)
        out[:, cols] = total.astype(BF16)

    wide = 2 * shard
    for c, pair in enumerate(chunks):
        landed(got.at[pair], x_recv.at[c])
        if wide % 128 == 0:
            settle(pair, pl.ds(pl.multiple_of(pair * wide, wide), wide))
    if wide % 128:
        for k in range(pairs):
            settle(k, slice(k * wide, (k + 1) * wide))
    for w in range(6):
        gone(rows_of(w, (pairs - 1) * shard), ring_send.at[w])
        gone(rows_of(w, pairs * shard), sib_send.at[w])
    gone(near.at[pl.ds(0, inner - 1)], near_send)
    gone(halo_src, halo_send)
    gone(got, x_send)
    for s, other in enumerate(far_peers, 1):

        @pl.when(layer + s < outer)
        def _():
            remote(total_map, far.at[layer], far_send.at[s - 1], far_recv.at[s - 1], other).wait_send()

        @pl.when(last)
        def _():
            remote(fin_src, fin_dst, fin_send.at[s - 1], fin_recv, other).wait_send()


def body(tokens, norm_gain, w_state_in, w_value, w_outer, w_inner, w_state_out, w_conv_out, log_step, decay_real, frequency, step_rate, input_real, input_imag, read_real, read_imag, skip_gain, conv_taps, initial_state):
    rows, features = tokens.shape[1:]
    groups, states = decay_real.shape
    group = skip_gain.shape[1]
    flat = groups * states
    channels = groups * group
    conv = conv_taps.shape[1]
    n_sp, n_fs, n_tp = (lax.axis_size(a) for a in ("sp", "fs", "tp"))
    shard = w_state_in.shape[0]
    pairs = n_sp * n_fs // 2
    half = pairs // 2
    inner = math.gcd(n_sp, 4)
    outer = n_sp // inner
    share = states // n_sp
    parts = pieces_of(shard)
    rest = (
        tokens[0], norm_gain[None], log_step[None], decay_real, frequency, step_rate,
        jnp.swapaxes(input_real, 1, 2).reshape(channels, states), jnp.swapaxes(input_imag, 1, 2).reshape(channels, states),
        read_real.reshape(channels, states), read_imag.reshape(channels, states), skip_gain.T, conv_taps,
        initial_state.reshape(2 * groups, states),
    )
    vmem = pltpu.VMEM
    dma = pltpu.SemaphoreType.DMA
    out, final = pl.pallas_call(
        lambda *refs: layer_kernel((n_sp, n_fs, n_tp, group, states), *refs),
        out_shape=(jax.ShapeDtypeStruct((rows // n_tp, features), BF16), jax.ShapeDtypeStruct((2, share, groups), F32)),
        in_specs=[pl.BlockSpec(memory_space=pl.ANY)] * 19,
        out_specs=[pl.BlockSpec(memory_space=vmem)] * 2,
        scratch_shapes=[
            *[vmem(a.shape, a.dtype) for a in rest],
            vmem((6, n_sp * n_fs * shard, channels), BF16),
            vmem((rows, features), BF16),
            vmem((rows, channels), BF16),
            *[vmem((rows, flat), F32)] * 4,
            vmem((4, SUB, flat), F32),
            vmem((4, flat), F32),
            vmem((inner, 4, flat), F32),
            vmem((4, flat), F32),
            vmem((outer, 4, flat), F32),
            vmem((2, flat), F32),
            vmem((2, flat), F32),
            vmem((rows + HALO, conv), F32),
            vmem((HALO, conv), BF16),
            vmem((HALO, conv), BF16),
            vmem((rows, conv), BF16),
            vmem((rows, channels), BF16),
            vmem((pairs, rows, 2 * shard), BF16),
            vmem((pairs, n_tp - 1, rows // n_tp, 2 * shard), BF16),
            vmem((rows, 128), F32),
            vmem((2, flat), F32),
            vmem((2, flat), F32),
            *[vmem((channels, states), BF16)] * 4,
            vmem((1, channels), F32),
            dma((13,)),
            dma((6,)),
            dma((6,)),
            dma((6, half, parts)),
            dma((6,)),
            dma((SO + 1 + half,)),
            dma,
            dma,
            dma((outer - 1,)),
            dma((outer - 1,)),
            dma((outer - 1,)),
            dma,
            dma,
            dma((pairs,)),
            dma,
            dma,
        ],
        compiler_params=pltpu.CompilerParams(collective_id=0, has_side_effects=True, vmem_limit_bytes=60000 * 1024),
        name="layer",
    )(w_state_in, w_value, w_inner, w_outer, w_state_out, w_conv_out, *rest)
    return out[None], jnp.swapaxes(final, 1, 2)[None]


def solution(mesh):
    return jax.shard_map(
        body,
        mesh=mesh,
        in_specs=(
            P("fs", "sp", None),
            P(),
            P(("sp", "fs"), "tp"),
            P(("sp", "fs"), "tp"),
            P(("sp", "fs"), "tp"),
            P(("sp", "fs"), "tp"),
            P(("sp", "fs"), "tp"),
            P(("sp", "fs"), "tp"),
            P("tp"),
            P("tp", None),
            P("tp", None),
            P("fs", "sp"),
            P("tp", None, None),
            P("tp", None, None),
            P("tp", None, None),
            P("tp", None, None),
            P("tp", None),
            P(None, "tp"),
            P("fs", None, "tp", None),
        ),
        out_specs=(P("fs", ("sp", "tp"), None), P("fs", None, "tp", "sp")),
        check_vma=False,
    )
```

```python
import math

import jax
import jax.numpy as jnp
from jax import lax
from jax.experimental import pallas as pl
from jax.experimental.pallas import tpu as pltpu
from jax.sharding import PartitionSpec as P

F32 = jnp.float32
BF16 = jnp.bfloat16
SUB = 8
SIN = (3.1415925798055846, -5.16770686616794, 2.5500311935192803, -0.5980441939118888, 0.07721838615680923)
COS = (0.9999999997799038, -4.93480213707883, 4.058709159556464, -1.335212003052184, 0.2349373138245546, -0.024396324364378108)


def poly(coeffs, z):
    total = coeffs[-1]
    for c in coeffs[-2::-1]:
        total = total * z + c
    return total


def dot(a, b, dims=((1,), (0,))):
    return lax.dot_general(a, b, (dims, ((), ())), preferred_element_type=F32)


def iota(shape, dim):
    return lax.broadcasted_iota(jnp.int32, shape, dim)


def exact(a, b, dims=((1,), (0,))):
    return lax.dot_general(a, b, (dims, ((), ())), precision=lax.Precision.HIGHEST, preferred_element_type=F32)


def cmul(ar, ai, br, bi):
    return ar * br - ai * bi, ar * bi + ai * br


def permutation(rows):
    run = rows // SUB
    r, t = iota((rows, rows), 0), iota((rows, rows), 1)
    return jnp.where((r % SUB) * run + r // SUB == t, 1.0, 0.0).astype(BF16)


def spread(mat, block, width, span, group, states):
    chans = slice(block * width, (block + 1) * width)
    tile = jnp.where(iota((states, span), 0) == iota((states, span), 1) % states, 1.0, 0.0).astype(BF16)
    keep = iota((width, span), 0) // group == iota((width, span), 1) // states
    return jnp.where(keep, dot(mat[chans, :], tile), 0.0).astype(BF16)


def couple(block, state_p, in_r, in_i, dr_ref, di_ref, group, states):
    width = state_p.shape[1]
    span = width // group * states
    cols = slice(block * span, (block + 1) * span)
    for src, dst in ((in_r, dr_ref), (in_i, di_ref)):
        dst[:, cols] = dot(state_p, spread(src, block, width, span, group, states))


def scan_block(lo, span, rate, coef, hr, hi, ar, ai):
    cols = pl.ds(lo, span)
    run = rate.shape[0] // SUB
    reps = span // 128
    decay = jnp.broadcast_to(coef[0:1, cols], (SUB, span))
    turn = jnp.broadcast_to(coef[1:2, cols], (SUB, span))

    def one(j, carry):
        h_r, h_i, a_r, a_i = carry
        at = pl.ds(pl.multiple_of(j * SUB, SUB), SUB)
        r = jnp.concatenate([rate[at, :]] * reps, axis=1)
        u = r * turn
        f = u - jnp.floor(u + 0.5)
        z = f * f
        s = f * poly(SIN, z)
        c = poly(COS, z)
        grow = jnp.exp(r * decay)
        gs = 2.0 * grow * s
        b_r = grow - gs * s
        b_i = gs * c
        p_r, p_i = cmul(b_r - 1.0, b_i, hr[at, cols], hi[at, cols])
        m_r, m_i = cmul(b_r, b_i, h_r, h_i)
        h_r, h_i = m_r + p_r, m_i + p_i
        a_r, a_i = cmul(b_r, b_i, a_r, a_i)
        hr[at, cols] = h_r
        hi[at, cols] = h_i
        ar[at, cols] = a_r
        ai[at, cols] = a_i
        return h_r, h_i, a_r, a_i

    zero = jnp.zeros((SUB, span), F32)
    lax.fori_loop(0, run, one, (zero, zero, zero + 1.0, zero), unroll=2)


def chain_subs(hr, hi, ar, ai, pre, summ):
    rows, flat = hr.shape
    last = rows - SUB
    m_r, m_i = jnp.ones((1, flat), F32), jnp.zeros((1, flat), F32)
    v_r, v_i = jnp.zeros((1, flat), F32), jnp.zeros((1, flat), F32)
    for s in range(SUB):
        row = slice(s, s + 1)
        pre[0, row, :], pre[1, row, :], pre[2, row, :], pre[3, row, :] = m_r, m_i, v_r, v_i
        at = slice(last + s, last + s + 1)
        e_r, e_i = ar[at, :], ai[at, :]
        m_r, m_i = cmul(e_r, e_i, m_r, m_i)
        w_r, w_i = cmul(e_r, e_i, v_r, v_i)
        v_r, v_i = w_r + hr[at, :], w_i + hi[at, :]
    summ[0:1, :], summ[1:2, :], summ[2:3, :], summ[3:4, :] = m_r, m_i, v_r, v_i


def enter(g, s_r, s_i):
    t_r, t_i = cmul(g[0:1, :], g[1:2, :], s_r, s_i)
    return t_r + g[2:3, :], t_i + g[3:4, :]


def join(first, second):
    g_r, g_i = second[0:1, :], second[1:2, :]
    m_r, m_i = cmul(g_r, g_i, first[0:1, :], first[1:2, :])
    w_r, w_i = cmul(g_r, g_i, first[2:3, :], first[3:4, :])
    return jnp.concatenate([m_r, m_i, w_r + second[2:3, :], w_i + second[3:4, :]], axis=0)


def readout(block, width, state_p, enter, hr, hi, ar, ai, pre, rd_r, rd_i, skip, perm, out, group, states):
    span = width // group * states
    cols = slice(block * span, (block + 1) * span)
    chans = slice(block * width, (block + 1) * width)
    rows = hr.shape[0]
    run = rows // SUB
    e_r, e_i = cmul(pre[0, :, cols], pre[1, :, cols], enter[0][:, cols], enter[1][:, cols])
    e_r, e_i = e_r + pre[2, :, cols], e_i + pre[3, :, cols]
    g_r = spread(rd_r, block, width, span, group, states)
    g_i = spread(rd_i, block, width, span, group, states)

    def fixed(local, a, b, sign):
        a3, b3 = a[:, cols].reshape(run, SUB, span), b[:, cols].reshape(run, SUB, span)
        x, y = (e_r, e_i) if sign < 0 else (e_i, e_r)
        shift = a3 * x[None] + (b3 * y[None] if sign > 0 else -b3 * y[None])
        return (local[:, cols].reshape(run, SUB, span) + shift).reshape(rows, span).astype(BF16)

    total = dot(fixed(hr, ar, ai, -1), g_r, ((1,), (1,))) - dot(fixed(hi, ar, ai, 1), g_i, ((1,), (1,)))
    v = total + skip[:, chans] * state_p[:, chans].astype(F32)
    mix = 0.5 * v * (1.0 + jnp.tanh(0.7978845608 * (v + 0.044715 * (v * v * v))))
    out[:, chans] = dot(perm, mix.astype(BF16), ((0,), (0,))).astype(BF16)


def prepare_rates(step_rate, rate):
    rows = rate.shape[0]
    run = rows // SUB
    r, t = iota((rows, rows), 0), iota((rows, rows), 1)
    chosen = jnp.where((r % SUB) * run + r // SUB == t, jnp.broadcast_to(step_rate[...], (rows, rows)), 0.0)
    rate[...] = exact(chosen, jnp.ones((rows, 128), F32))


def flatten(parts, states):
    groups = parts[0].shape[0]
    flat = groups * states
    tile = jnp.where(iota((states, flat), 0) == iota((states, flat), 1) % states, 1.0, 0.0)
    keep = iota((groups, flat), 0) == iota((groups, flat), 1) // states
    return [jnp.sum(jnp.where(keep, exact(part, tile), 0.0), axis=0, keepdims=True) for part in parts]


def prepare_base(log_step, groups):
    base = jnp.where(iota((groups, groups), 0) == iota((groups, groups), 1), jnp.broadcast_to(jnp.exp(log_step[...]), (groups, groups)), 0.0)
    return jnp.sum(base, axis=1, keepdims=True)


def prepare_inverse(decay, frequency, group, scratch):
    groups = decay.shape[0]
    d, f = decay[...], frequency[...]
    modulus = d * d + f * f
    each = jnp.where(iota((groups * group, groups), 0) // group == iota((groups * group, groups), 1), 1.0, 0.0)
    scratch[0], scratch[1] = exact(each, d / modulus), exact(each, -f / modulus)


def prepare_inputs(inverse, input_real, input_imag, in_r, in_i):
    x_r, x_i = input_real[...], input_imag[...]
    in_r[...] = (x_r * inverse[0] - x_i * inverse[1]).astype(BF16)
    in_i[...] = (x_r * inverse[1] + x_i * inverse[0]).astype(BF16)


def prepare_skip(skip_gain, skip):
    group, groups = skip_gain.shape
    chans = groups * group
    each = jnp.where(iota((groups, chans), 0) == iota((groups, chans), 1) // group, 1.0, 0.0)
    keep = iota((group, chans), 0) == iota((group, chans), 1) % group
    skip[...] = jnp.sum(jnp.where(keep, exact(skip_gain[...], each), 0.0), axis=0, keepdims=True)


def own_states(row, sp, share, groups, states):
    flat = groups * states
    shape = (SUB, flat)
    mine = jnp.where(iota(shape, 1) % states == sp * share + iota(shape, 0), jnp.broadcast_to(row, shape), 0.0)
    each = jnp.where(iota((groups, flat), 0) == iota((groups, flat), 1) // states, 1.0, 0.0)
    return exact(mine, each, ((1,), (1,)))[0:share, :]


MESH = pl.DeviceIdType.MESH
HALO = 16
AHEAD = 4


def pieces_of(shard):
    return 2 if shard >= 64 else 1


S, V, I, O, SO, CO = range(6)


def layer_kernel(sizes, *refs):
    n_sp, n_fs, n_tp, group, states = sizes
    inputs, (out, final), scratch = refs[:19], refs[19:21], refs[21:]
    hbm_weights, hbm_rest = inputs[:6], inputs[6:]
    local, scratch = scratch[:13], scratch[13:]
    (
        full, normed, state_p, hr, hi, ar, ai, pre, level, near, inbox, fin_src, fin_dst, ext, halo,
        conv_mix, state_mix, partial, got, rate, coef, opening, in_r, in_i, rd_r, rd_i, skip, inverse,
        load, load_w, ring_send, ring_recv, sib_send, sib_recv, near_send, near_recv, chain_send, chain_recv, fin_send, fin_recv,
        x_send, x_recv, halo_send, halo_recv, mix_send, mix_recv,
    ) = scratch
    tokens, gain, log_step, decay, frequency, step_rate, input_real, input_imag, read_real, read_imag, skip_gain, taps, initial = local
    shard = hbm_weights[0].shape[0]
    rows = tokens.shape[0]
    channels = hbm_weights[0].shape[1]
    sp, fs, tp = lax.axis_index("sp"), lax.axis_index("fs"), lax.axis_index("tp")
    pairs = n_sp * n_fs // 2
    half = pairs // 2
    parts = pieces_of(shard)
    piece = shard // parts
    inner = math.gcd(n_sp, 4)
    outer = n_sp // inner
    here, layer = sp % inner, sp // inner
    mine = sp * n_fs + fs
    parity, chip = mine % 2, mine // 2
    place = jnp.where(chip % 2 == 0, chip // 2, pairs - 1 - chip // 2)

    def own(w):
        return full.at[w, pl.ds(pl.multiple_of(mine * shard, shard), shard), :]

    loads = [pltpu.make_async_copy(src, own(w), load_w.at[w]) for w, src in enumerate(hbm_weights)]
    rest = [pltpu.make_async_copy(src, dst, load.at[k]) for k, (src, dst) in enumerate(zip(hbm_rest, local))]
    for copy in loads[:2] + rest[:1] + loads[2:] + rest[1:]:
        copy.start()

    def pair_at(offset):
        q = (place + offset + pairs) % pairs
        return jnp.where(q < half, q * 2, (pairs - 1 - q) * 2 + 1)

    def device(linear):
        return (linear // n_fs, linear % n_fs, tp)

    neighbours = (device(pair_at(1) * 2 + parity), device(pair_at(-1) * 2 + parity))
    sibling = device(chip * 2 + 1 - parity)
    stages = inner.bit_length() - 1
    late = [(here >> k) % 2 == 1 for k in range(stages)]
    near_peers = [(sp + jnp.where(late[k], -1, 1) * (1 << k), fs, tp) for k in range(stages)]
    above = ((sp + inner) % n_sp, fs, tp)
    below = [(sp - s * inner + n_sp) % n_sp for s in range(1, outer)]
    after = ((sp + 1) % n_sp, fs, tp)
    tp_peers = [(sp, fs, (tp + s) % n_tp) for s in range(1, n_tp)]

    barrier = pltpu.get_barrier_semaphore()
    across = [(sibling[0], sibling[1], (tp + s) % n_tp) for s in range(n_tp)]
    greet = list(neighbours) + tp_peers + across
    for other in greet:
        pl.semaphore_signal(barrier, inc=1, device_id=other, device_id_type=MESH)
    pl.semaphore_wait(barrier, len(greet))

    def remote(src, dst, s_sem, r_sem, to):
        return pltpu.make_async_remote_copy(src_ref=src, dst_ref=dst, send_sem=s_sem, recv_sem=r_sem, device_id=to, device_id_type=MESH)

    def send(src, dst, s_sem, r_sem, to):
        remote(src, dst, s_sem, r_sem, to).start()

    def landed(ref, r_sem):
        remote(ref, ref, r_sem, r_sem, sibling).wait_recv()

    def gone(ref, s_sem):
        remote(ref, ref, s_sem, s_sem, sibling).wait_send()

    def slot(w, pair, par, h):
        return full.at[w, pl.ds(pl.multiple_of((pair * 2 + par) * shard + h * piece, piece), piece), :]

    def rounds(w, way):
        return half if way == w % 2 else pairs - 1 - half

    def source(way, r):
        return pair_at(-1 - r if way == 0 else 1 + r)

    def ways(w, r):
        return [way for way in range(2) if r < rounds(w, way)]

    def rows_of(w, count):
        return full.at[w, pl.ds(0, count), :]

    last_round = half - 1
    filler = [(V, r, h) for r in range(half) for h in range(parts)]
    pieces = []
    for r in range(half):
        pieces += [(S, r, h) for h in range(parts)] + filler[:1]
        del filler[:1]
    outputs = [(w, r) for r in range(half) for w in (SO, CO)]

    def both(*units):
        return [(w, r, h) for w, r in units for h in range(parts)]

    for r in range(half):
        if r < last_round:
            pieces += both((I, r), (O, r)) + filler[:parts]
            del filler[:parts]
        else:
            pieces += filler + both(outputs[0], (I, r), (O, r), *outputs[1:])
    where = {item: k for k, item in enumerate(pieces)}
    sent_to, seen = [0], [0]

    def send_piece(w, r, h):
        if r == 0 and h == 0:
            loads[w].wait()
        for way in ways(w, r):
            at = chip if r == 0 else source(way, r - 1)
            ref = slot(w, at, parity, h)
            send(ref, ref, ring_send.at[w], ring_recv.at[w, r, h], neighbours[way])
        if r == 0 and h == parts - 1 and w < SO:
            send(own(w), own(w), sib_send.at[w], sib_recv.at[w], sibling)

    def feed():
        while sent_to[0] < len(pieces) and sent_to[0] <= seen[0] + AHEAD:
            w, r, h = pieces[sent_to[0]]
            if r > 0 and where[w, r - 1, h] >= seen[0]:
                break
            send_piece(w, r, h)
            sent_to[0] += 1

    def pump(count=1):
        for _ in range(count):
            if seen[0] == len(pieces):
                return
            w, r, h = pieces[seen[0]]
            landed(rows_of(w, len(ways(w, r)) * piece), ring_recv.at[w, r, h])
            seen[0] += 1
            feed()
            for way in ways(w, r) if w < SO else ():
                ref = slot(w, source(way, r), parity, h)
                send(ref, ref, sib_send.at[w], sib_recv.at[w], sibling)

    def until(w, r):
        pump(max(0, where[w, r, parts - 1] + 1 - seen[0]))

    def finish(w):
        until(w, last_round)
        landed(rows_of(w, pairs * shard), sib_recv.at[w])

    feed()
    rest[0].wait()
    rest[1].wait()

    def normalize(x):
        x = x.astype(F32)
        scale = lax.rsqrt(jnp.mean(x * x, axis=-1, keepdims=True) + 1e-06)
        return (x * scale * gain[...]).astype(BF16)

    def norm(j, carry):
        at = pl.multiple_of(j * 32, 32)
        normed[pl.ds(HALO + at, 32), :] = normalize(tokens[pl.ds(at, 32), :])
        return carry

    lax.fori_loop(0, rows // 32, norm, 0)
    for copy in rest[2:]:
        copy.wait()
    pump()
    perm = permutation(rows)
    prepare_rates(step_rate, rate)
    pump()
    prepare_inverse(decay, frequency, group, inverse)
    pump()
    prepare_inputs(inverse, input_real, input_imag, in_r, in_i)
    pump()
    base = prepare_base(log_step, decay.shape[0])
    coef[0:1, :], coef[1:2, :] = flatten([base * decay[...], base * frequency[...] * 0.15915494309189535], states)
    pump()
    opening[0:1, :], opening[1:2, :] = flatten([initial[0 : decay.shape[0], :], initial[decay.shape[0] :, :]], states)
    pump()
    rd_r[...] = read_real[...].astype(BF16)
    rd_i[...] = read_imag[...].astype(BF16)
    prepare_skip(skip_gain, skip)
    finish(S)

    def project(w):
        return dot(normed[HALO:, :], full[w]).astype(BF16)

    def project_more(w):
        return dot(normed[...], full[w]).astype(BF16)

    send(tokens.at[pl.ds(rows - SUB, SUB), :], halo, halo_send, halo_recv, after)
    state_p[...] = dot(perm, project(S)).astype(BF16)
    pump(2)
    width = min(128, channels)
    span = width // group * states
    blocks = channels // width
    for block in range(blocks):
        couple(block, state_p[:, block * width : (block + 1) * width], in_r, in_i, hr, hi, group, states)
        scan_block(block * span, span, rate, coef, hr, hi, ar, ai)
        pump(1 + block % 2)
    chain_subs(hr, hi, ar, ai, pre, level.at[0])

    def meet(k):
        landed(near.at[k], near_recv.at[k])
        mine_k, theirs = level[k], near[k]
        level[k + 1] = join(jnp.where(late[k], theirs, mine_k), jnp.where(late[k], mine_k, theirs))

    def carry_on(t):
        @pl.when(layer == t)
        def _():
            if t > 0:
                landed(inbox, chain_recv)
            start = inbox if t > 0 else opening
            fin_src[0:1, :], fin_src[1:2, :] = enter(level[stages], start[0:1, :], start[1:2, :])
            if t < outer - 1:
                remote(fin_src, inbox, chain_send, chain_recv, above).start()
            else:
                for s, other in enumerate(below):
                    remote(fin_src, fin_dst, fin_send.at[s], fin_recv, (other, fs, tp)).start()

    for k in range(stages):
        send(level.at[k], near.at[k], near_send.at[k], near_recv.at[k], near_peers[k])
        pump(2 + k)
        meet(k)
    carry_on(0)
    pump(2)
    landed(halo, halo_recv)
    normed[:HALO, :] = jnp.concatenate([jnp.zeros((HALO - SUB, halo.shape[1]), BF16), normalize(halo[...])], axis=0)
    finish(V)
    value = project_more(V)
    for t in range(1, outer - 1):
        carry_on(t)
        pump(3)
    finish(I)
    product = project_more(I).astype(F32) * value.astype(F32)
    product = jnp.where(jnp.logical_and(sp == 0, iota(product.shape, 0) < HALO), 0.0, product)
    ext[...] = product.astype(BF16).astype(F32)
    pump()
    for t in range(max(1, outer - 1), outer):
        carry_on(t)
    last = layer == outer - 1
    e_r = jnp.where(layer == 0, opening[0:1, :], inbox[0:1, :])
    e_i = jnp.where(layer == 0, opening[1:2, :], inbox[1:2, :])
    for k in reversed(range(stages)):
        t_r, t_i = enter(near[k], e_r, e_i)
        e_r, e_i = jnp.where(late[k], t_r, e_r), jnp.where(late[k], t_i, e_i)
    for block in range(blocks):
        readout(block, width, state_p, (e_r, e_i), hr, hi, ar, ai, pre, rd_r, rd_i, skip, perm, state_mix.at[parity], group, states)
        if block % 2 == 1:
            pump()

    send(state_mix.at[parity], state_mix.at[parity], mix_send.at[0], mix_recv.at[0], sibling)
    finish(O)
    outward = project(O)
    reach = taps.shape[0] - 1
    filtered = taps[0:1, :] * ext[HALO - reach : HALO - reach + rows, :]
    for tap in range(1, reach + 1):
        at = HALO - reach + tap
        filtered = filtered + taps[tap : tap + 1, :] * ext[at : at + rows, :]
    conv_mix[parity] = (outward.astype(F32) * filtered).astype(BF16)
    pump()
    send(conv_mix.at[parity], conv_mix.at[parity], mix_send.at[1], mix_recv.at[1], sibling)
    own_rows = rows // n_tp
    chunks = []

    def columns(pair, par):
        return pl.ds(pl.multiple_of((pair * 2 + par) * shard, shard), shard)

    def compute(some):
        mixes = [(mix[...].reshape(2 * rows, mix.shape[2]), w) for mix, w in ((state_mix, SO), (conv_mix, CO))]
        total = 0.0
        for mix, w in mixes:
            total = total + dot(mix, jnp.concatenate([full[w, columns(pair, parity), :] for pair in some], axis=0), ((1,), (1,)))
        total = total.astype(BF16)
        for k, pair in enumerate(some):
            partial[pl.ds(pair, 1)] = total[:, k * shard : (k + 1) * shard][None]

    def exchange(pair):
        for s in range(n_tp):
            for core in range(2):
                if s + core > 0:
                    other = (tp + s) % n_tp
                    at = (parity if core == 0 else 1 - parity) * rows + other * own_rows
                    theirs = partial.at[pair, pl.ds(pl.multiple_of(at, own_rows), own_rows), :]
                    to = across[s] if core else (sp, fs, other)
                    send(theirs, got.at[pair, core * (n_tp - 1) + s - 1 + core], x_send, x_recv.at[len(chunks)], to)
        chunks.append(pair)

    for k, mix in enumerate((state_mix, conv_mix)):
        landed(mix.at[1 - parity], mix_recv.at[k])
    compute([chip])
    exchange(chip)
    for r in range(half):
        until(SO, r)
        until(CO, r)
        fresh = [source(way, r) for way in ways(SO, r) if r < last_round or way == 0]
        compute(fresh)
        for pair in fresh:
            exchange(pair)
        pump()

    @pl.when(jnp.logical_not(last))
    def _():
        landed(fin_dst, fin_recv)

    share_states = states // n_sp
    groups = decay.shape[0]
    for k in range(2):
        row = jnp.where(last, fin_src[k : k + 1, :], fin_dst[k : k + 1, :])
        final[k] = own_states(row, sp, share_states, groups, states)
    kept = pl.ds(pl.multiple_of(parity * rows + tp * own_rows, own_rows), own_rows)

    def settle(k):
        ours, theirs = partial[k, kept, :].astype(F32), got[k, n_tp - 1].astype(F32)
        for s in range(1, n_tp):
            ours = ours + got[k, s - 1].astype(F32)
            theirs = theirs + got[k, n_tp - 1 + s].astype(F32)
        return ours.astype(BF16), theirs.astype(BF16)

    for c, pair in enumerate(chunks):
        landed(got.at[pair], x_recv.at[c])
        if shard % 128 == 0:
            out[:, columns(pair, parity)], out[:, columns(pair, 1 - parity)] = settle(pair)
    if shard % 128:
        for k in range(pairs):
            ours, theirs = settle(k)
            out[:, k * 2 * shard : (k * 2 + 1) * shard] = jnp.where(parity == 0, ours, theirs)
            out[:, (k * 2 + 1) * shard : (k + 1) * 2 * shard] = jnp.where(parity == 0, theirs, ours)
    for w in range(6):
        gone(rows_of(w, (pairs - 1) * shard), ring_send.at[w])
        if w < SO:
            gone(rows_of(w, pairs * shard), sib_send.at[w])
    for k in range(stages):
        gone(near.at[k], near_send.at[k])
    gone(halo, halo_send)
    gone(got, x_send)
    for k, mix in enumerate((state_mix, conv_mix)):
        gone(mix.at[parity], mix_send.at[k])

    @pl.when(jnp.logical_not(last))
    def _():
        gone(fin_src, chain_send)

    for s in range(outer - 1):

        @pl.when(last)
        def _():
            gone(fin_src, fin_send.at[s])


def body(tokens, norm_gain, w_state_in, w_value, w_outer, w_inner, w_state_out, w_conv_out, log_step, decay_real, frequency, step_rate, input_real, input_imag, read_real, read_imag, skip_gain, conv_taps, initial_state):
    rows, features = tokens.shape[1:]
    groups, states = decay_real.shape
    group = skip_gain.shape[1]
    flat = groups * states
    channels = groups * group
    conv = conv_taps.shape[1]
    n_sp, n_fs, n_tp = (lax.axis_size(a) for a in ("sp", "fs", "tp"))
    shard = w_state_in.shape[0]
    pairs = n_sp * n_fs // 2
    half = pairs // 2
    inner = math.gcd(n_sp, 4)
    outer = n_sp // inner
    share = states // n_sp
    parts = pieces_of(shard)
    rest = (
        tokens[0], norm_gain[None], log_step[None], decay_real, frequency, step_rate,
        jnp.swapaxes(input_real, 1, 2).reshape(channels, states), jnp.swapaxes(input_imag, 1, 2).reshape(channels, states),
        read_real.reshape(channels, states), read_imag.reshape(channels, states), skip_gain.T, conv_taps,
        initial_state.reshape(2 * groups, states),
    )
    vmem = pltpu.VMEM
    dma = pltpu.SemaphoreType.DMA
    out, final = pl.pallas_call(
        lambda *refs: layer_kernel((n_sp, n_fs, n_tp, group, states), *refs),
        out_shape=(jax.ShapeDtypeStruct((rows // n_tp, features), BF16), jax.ShapeDtypeStruct((2, share, groups), F32)),
        in_specs=[pl.BlockSpec(memory_space=pl.ANY)] * 19,
        out_specs=[pl.BlockSpec(memory_space=vmem)] * 2,
        scratch_shapes=[
            *[vmem(a.shape, a.dtype) for a in rest],
            vmem((6, n_sp * n_fs * shard, channels), BF16),
            vmem((HALO + rows, features), BF16),
            vmem((rows, channels), BF16),
            *[vmem((rows, flat), F32)] * 4,
            vmem((4, SUB, flat), F32),
            vmem((inner.bit_length(), 4, flat), F32),
            vmem((inner.bit_length() - 1, 4, flat), F32),
            vmem((2, flat), F32),
            vmem((2, flat), F32),
            vmem((2, flat), F32),
            vmem((rows + HALO, conv), F32),
            vmem((SUB, features), BF16),
            vmem((2, rows, conv), BF16),
            vmem((2, rows, channels), BF16),
            vmem((pairs, 2 * rows, shard), BF16),
            vmem((pairs, 2 * n_tp - 1, rows // n_tp, shard), BF16),
            vmem((rows, 128), F32),
            vmem((2, flat), F32),
            vmem((2, flat), F32),
            *[vmem((channels, states), BF16)] * 4,
            vmem((1, channels), F32),
            vmem((2, channels, states), F32),
            dma((13,)),
            dma((6,)),
            dma((6,)),
            dma((6, half, parts)),
            dma((SO,)),
            dma((SO,)),
            dma((inner.bit_length() - 1,)),
            dma((inner.bit_length() - 1,)),
            dma,
            dma,
            dma((outer - 1,)),
            dma,
            dma,
            dma((pairs,)),
            dma,
            dma,
            dma((2,)),
            dma((2,)),
        ],
        compiler_params=pltpu.CompilerParams(collective_id=0, has_side_effects=True, vmem_limit_bytes=60000 * 1024),
        name="layer",
    )(w_state_in, w_value, w_inner, w_outer, w_state_out, w_conv_out, *rest)
    return out[None], jnp.swapaxes(final, 1, 2)[None]


def solution(mesh):
    return jax.shard_map(
        body,
        mesh=mesh,
        in_specs=(
            P("fs", "sp", None),
            P(),
            P(("sp", "fs"), "tp"),
            P(("sp", "fs"), "tp"),
            P(("sp", "fs"), "tp"),
            P(("sp", "fs"), "tp"),
            P(("sp", "fs"), "tp"),
            P(("sp", "fs"), "tp"),
            P("tp"),
            P("tp", None),
            P("tp", None),
            P("fs", "sp"),
            P("tp", None, None),
            P("tp", None, None),
            P("tp", None, None),
            P("tp", None, None),
            P("tp", None),
            P(None, "tp"),
            P("fs", None, "tp", None),
        ),
        out_specs=(P("fs", ("sp", "tp"), None), P("fs", None, "tp", "sp")),
        check_vma=False,
    )
```

```python
import math

import jax
import jax.numpy as jnp
from jax import lax
from jax.experimental import pallas as pl
from jax.experimental.pallas import tpu as pltpu
from jax.sharding import PartitionSpec as P

F32 = jnp.float32
BF16 = jnp.bfloat16
SUB = 8
SIN = (3.1415925798055846, -5.16770686616794, 2.5500311935192803, -0.5980441939118888, 0.07721838615680923)
COS = (0.9999999997799038, -4.93480213707883, 4.058709159556464, -1.335212003052184, 0.2349373138245546, -0.024396324364378108)


def poly(coeffs, z):
    total = coeffs[-1]
    for c in coeffs[-2::-1]:
        total = total * z + c
    return total


def dot(a, b, dims=((1,), (0,))):
    return lax.dot_general(a, b, (dims, ((), ())), preferred_element_type=F32)


def iota(shape, dim):
    return lax.broadcasted_iota(jnp.int32, shape, dim)


def exact(a, b, dims=((1,), (0,))):
    return lax.dot_general(a, b, (dims, ((), ())), precision=lax.Precision.HIGHEST, preferred_element_type=F32)


def cmul(ar, ai, br, bi):
    return ar * br - ai * bi, ar * bi + ai * br


def permutation(rows):
    run = rows // SUB
    r, t = iota((rows, rows), 0), iota((rows, rows), 1)
    return jnp.where((r % SUB) * run + r // SUB == t, 1.0, 0.0).astype(BF16)


def spread(mat, block, width, span, group, states):
    chans = slice(block * width, (block + 1) * width)
    tile = jnp.where(iota((states, span), 0) == iota((states, span), 1) % states, 1.0, 0.0).astype(BF16)
    keep = iota((width, span), 0) // group == iota((width, span), 1) // states
    return jnp.where(keep, dot(mat[chans, :], tile), 0.0).astype(BF16)


def couple(block, state_p, in_r, in_i, dr_ref, di_ref, group, states):
    width = state_p.shape[1]
    span = width // group * states
    cols = slice(block * span, (block + 1) * span)
    for src, dst in ((in_r, dr_ref), (in_i, di_ref)):
        dst[:, cols] = dot(state_p, spread(src, block, width, span, group, states))


def scan_block(lo, span, rate, coef, hr, hi, ar, ai):
    cols = pl.ds(lo, span)
    run = rate.shape[0] // SUB
    reps = span // 128
    decay = jnp.broadcast_to(coef[0:1, cols], (SUB, span))
    turn = jnp.broadcast_to(coef[1:2, cols], (SUB, span))

    def one(j, carry):
        h_r, h_i, a_r, a_i = carry
        at = pl.ds(pl.multiple_of(j * SUB, SUB), SUB)
        r = jnp.concatenate([rate[at, :]] * reps, axis=1)
        u = r * turn
        f = u - jnp.floor(u + 0.5)
        z = f * f
        s = f * poly(SIN, z)
        c = poly(COS, z)
        grow = jnp.exp(r * decay)
        gs = 2.0 * grow * s
        b_r = grow - gs * s
        b_i = gs * c
        p_r, p_i = cmul(b_r - 1.0, b_i, hr[at, cols], hi[at, cols])
        m_r, m_i = cmul(b_r, b_i, h_r, h_i)
        h_r, h_i = m_r + p_r, m_i + p_i
        a_r, a_i = cmul(b_r, b_i, a_r, a_i)
        hr[at, cols] = h_r
        hi[at, cols] = h_i
        ar[at, cols] = a_r
        ai[at, cols] = a_i
        return h_r, h_i, a_r, a_i

    zero = jnp.zeros((SUB, span), F32)
    lax.fori_loop(0, run, one, (zero, zero, zero + 1.0, zero), unroll=2)


def chain_subs(hr, hi, ar, ai, pre, summ):
    rows, flat = hr.shape
    last = rows - SUB
    m_r, m_i = jnp.ones((1, flat), F32), jnp.zeros((1, flat), F32)
    v_r, v_i = jnp.zeros((1, flat), F32), jnp.zeros((1, flat), F32)
    for s in range(SUB):
        row = slice(s, s + 1)
        pre[0, row, :], pre[1, row, :], pre[2, row, :], pre[3, row, :] = m_r, m_i, v_r, v_i
        at = slice(last + s, last + s + 1)
        e_r, e_i = ar[at, :], ai[at, :]
        m_r, m_i = cmul(e_r, e_i, m_r, m_i)
        w_r, w_i = cmul(e_r, e_i, v_r, v_i)
        v_r, v_i = w_r + hr[at, :], w_i + hi[at, :]
    summ[0:1, :], summ[1:2, :], summ[2:3, :], summ[3:4, :] = m_r, m_i, v_r, v_i


def enter(g, s_r, s_i):
    t_r, t_i = cmul(g[0:1, :], g[1:2, :], s_r, s_i)
    return t_r + g[2:3, :], t_i + g[3:4, :]


def join(first, second):
    g_r, g_i = second[0:1, :], second[1:2, :]
    m_r, m_i = cmul(g_r, g_i, first[0:1, :], first[1:2, :])
    w_r, w_i = cmul(g_r, g_i, first[2:3, :], first[3:4, :])
    return jnp.concatenate([m_r, m_i, w_r + second[2:3, :], w_i + second[3:4, :]], axis=0)


def readout(block, width, state_p, enter, hr, hi, ar, ai, pre, rd_r, rd_i, skip, perm, out, group, states):
    span = width // group * states
    cols = slice(block * span, (block + 1) * span)
    chans = slice(block * width, (block + 1) * width)
    rows = hr.shape[0]
    run = rows // SUB
    e_r, e_i = cmul(pre[0, :, cols], pre[1, :, cols], enter[0][:, cols], enter[1][:, cols])
    e_r, e_i = e_r + pre[2, :, cols], e_i + pre[3, :, cols]
    g_r = spread(rd_r, block, width, span, group, states)
    g_i = spread(rd_i, block, width, span, group, states)

    def fixed(local, a, b, sign):
        a3, b3 = a[:, cols].reshape(run, SUB, span), b[:, cols].reshape(run, SUB, span)
        x, y = (e_r, e_i) if sign < 0 else (e_i, e_r)
        shift = a3 * x[None] + (b3 * y[None] if sign > 0 else -b3 * y[None])
        return (local[:, cols].reshape(run, SUB, span) + shift).reshape(rows, span).astype(BF16)

    total = dot(fixed(hr, ar, ai, -1), g_r, ((1,), (1,))) - dot(fixed(hi, ar, ai, 1), g_i, ((1,), (1,)))
    v = total + skip[:, chans] * state_p[:, chans].astype(F32)
    mix = 0.5 * v * (1.0 + jnp.tanh(0.7978845608 * (v + 0.044715 * (v * v * v))))
    out[:, chans] = dot(perm, mix.astype(BF16), ((0,), (0,))).astype(BF16)


def prepare_rates(step_rate, rate):
    rows = rate.shape[0]
    run = rows // SUB
    r, t = iota((rows, rows), 0), iota((rows, rows), 1)
    chosen = jnp.where((r % SUB) * run + r // SUB == t, jnp.broadcast_to(step_rate[...], (rows, rows)), 0.0)
    rate[...] = exact(chosen, jnp.ones((rows, 128), F32))


def flatten(parts, states):
    groups = parts[0].shape[0]
    flat = groups * states
    tile = jnp.where(iota((states, flat), 0) == iota((states, flat), 1) % states, 1.0, 0.0)
    keep = iota((groups, flat), 0) == iota((groups, flat), 1) // states
    return [jnp.sum(jnp.where(keep, exact(part, tile), 0.0), axis=0, keepdims=True) for part in parts]


def prepare_base(log_step, groups):
    base = jnp.where(iota((groups, groups), 0) == iota((groups, groups), 1), jnp.broadcast_to(jnp.exp(log_step[...]), (groups, groups)), 0.0)
    return jnp.sum(base, axis=1, keepdims=True)


def prepare_inverse(decay, frequency, group, scratch):
    groups = decay.shape[0]
    d, f = decay[...], frequency[...]
    modulus = d * d + f * f
    each = jnp.where(iota((groups * group, groups), 0) // group == iota((groups * group, groups), 1), 1.0, 0.0)
    scratch[0], scratch[1] = exact(each, d / modulus), exact(each, -f / modulus)


def prepare_inputs(inverse, input_real, input_imag, in_r, in_i):
    x_r, x_i = input_real[...], input_imag[...]
    in_r[...] = (x_r * inverse[0] - x_i * inverse[1]).astype(BF16)
    in_i[...] = (x_r * inverse[1] + x_i * inverse[0]).astype(BF16)


def prepare_skip(skip_gain, skip):
    group, groups = skip_gain.shape
    chans = groups * group
    each = jnp.where(iota((groups, chans), 0) == iota((groups, chans), 1) // group, 1.0, 0.0)
    keep = iota((group, chans), 0) == iota((group, chans), 1) % group
    skip[...] = jnp.sum(jnp.where(keep, exact(skip_gain[...], each), 0.0), axis=0, keepdims=True)


def own_states(row, sp, share, groups, states):
    flat = groups * states
    shape = (SUB, flat)
    mine = jnp.where(iota(shape, 1) % states == sp * share + iota(shape, 0), jnp.broadcast_to(row, shape), 0.0)
    each = jnp.where(iota((groups, flat), 0) == iota((groups, flat), 1) // states, 1.0, 0.0)
    return exact(mine, each, ((1,), (1,)))[0:share, :]


MESH = pl.DeviceIdType.MESH
HALO = 16
AHEAD = 5
SLOTS = 16


def pieces_of(shard):
    return 2 if shard >= 64 else 1


S, V, I, O, SO, CO = range(6)


def layer_kernel(sizes, *refs):
    n_sp, n_fs, n_tp, group, states = sizes
    inputs, (out, final), scratch = refs[:19], refs[19:21], refs[21:]
    hbm_weights, hbm_rest = inputs[:6], inputs[6:]
    local, scratch = scratch[:13], scratch[13:]
    (
        full, normed, state_p, hr, hi, ar, ai, pre, level, near, inbox, passed, reach_map, fin_src, fin_dst, ext, halo,
        conv_mix, state_mix, partial, got, rate, coef, opening, in_r, in_i, rd_r, rd_i, skip, inverse,
        load, load_w, ring_send, ring_recv, sib_send, sib_recv, near_send, near_recv, chain_send, chain_recv, map_send, map_recv, fin_send, fin_recv,
        x_send, x_recv, halo_send, halo_recv, mix_send, mix_recv,
    ) = scratch
    tokens, gain, log_step, decay, frequency, step_rate, input_real, input_imag, read_real, read_imag, skip_gain, taps, initial = local
    shard = hbm_weights[0].shape[0]
    rows = tokens.shape[0]
    channels = hbm_weights[0].shape[1]
    sp, fs, tp = lax.axis_index("sp"), lax.axis_index("fs"), lax.axis_index("tp")
    pairs = n_sp * n_fs // 2
    half = pairs // 2
    parts = pieces_of(shard)
    piece = shard // parts
    inner = math.gcd(n_sp, 4)
    outer = n_sp // inner
    here, layer = sp % inner, sp // inner
    mine = sp * n_fs + fs
    parity, chip = mine % 2, mine // 2
    place = jnp.where(chip % 2 == 0, chip // 2, pairs - 1 - chip // 2)

    def own(w):
        return full.at[w, pl.ds(pl.multiple_of(mine * shard, shard), shard), :]

    loads = [pltpu.make_async_copy(src, own(w), load_w.at[w]) for w, src in enumerate(hbm_weights)]
    rest = [pltpu.make_async_copy(src, dst, load.at[k]) for k, (src, dst) in enumerate(zip(hbm_rest, local))]
    for copy in loads[:2] + rest[:1] + loads[2:] + rest[1:]:
        copy.start()

    def pair_at(offset):
        q = (place + offset + pairs) % pairs
        return jnp.where(q < half, q * 2, (pairs - 1 - q) * 2 + 1)

    def device(linear):
        return (linear // n_fs, linear % n_fs, tp)

    neighbours = (device(pair_at(1) * 2 + parity), device(pair_at(-1) * 2 + parity))
    sibling = device(chip * 2 + 1 - parity)
    stages = inner.bit_length() - 1
    late = [(here >> k) % 2 == 1 for k in range(stages)]
    near_peers = [(sp + jnp.where(late[k], -1, 1) * (1 << k), fs, tp) for k in range(stages)]
    above = ((sp + inner) % n_sp, fs, tp)
    below = [(sp - s * inner + n_sp) % n_sp for s in range(1, outer)]
    after = ((sp + 1) % n_sp, fs, tp)
    tp_peers = [(sp, fs, (tp + s) % n_tp) for s in range(1, n_tp)]

    barrier = pltpu.get_barrier_semaphore()
    across = [(sibling[0], sibling[1], (tp + s) % n_tp) for s in range(n_tp)]
    greet = list(neighbours) + tp_peers + across
    for other in greet:
        pl.semaphore_signal(barrier, inc=1, device_id=other, device_id_type=MESH)
    pl.semaphore_wait(barrier, len(greet))

    def remote(src, dst, s_sem, r_sem, to):
        return pltpu.make_async_remote_copy(src_ref=src, dst_ref=dst, send_sem=s_sem, recv_sem=r_sem, device_id=to, device_id_type=MESH)

    def send(src, dst, s_sem, r_sem, to):
        remote(src, dst, s_sem, r_sem, to).start()

    def landed(ref, r_sem):
        remote(ref, ref, r_sem, r_sem, sibling).wait_recv()

    def gone(ref, s_sem):
        remote(ref, ref, s_sem, s_sem, sibling).wait_send()

    def slot(w, pair, par, h):
        return full.at[w, pl.ds(pl.multiple_of((pair * 2 + par) * shard + h * piece, piece), piece), :]

    def rounds(w, way):
        return half if way == w % 2 else pairs - 1 - half

    def source(way, r):
        return pair_at(-1 - r if way == 0 else 1 + r)

    def ways(w, r):
        return [way for way in range(2) if r < rounds(w, way)]

    def rows_of(w, count):
        return full.at[w, pl.ds(0, count), :]

    last_round = half - 1
    filler = [(V, r, h) for r in range(half) for h in range(parts)]
    pieces = []
    for r in range(half):
        pieces += [(S, r, h) for h in range(parts)] + filler[:1]
        del filler[:1]
    outputs = [(w, r) for r in range(half) for w in (SO, CO)]

    def both(*units):
        return [(w, r, h) for w, r in units for h in range(parts)]

    for r in range(half):
        if r < last_round:
            pieces += both((I, r), (O, r)) + filler[:parts]
            del filler[:parts]
        else:
            pieces += filler + both(outputs[0], (I, r), (O, r), *outputs[1:])
    where = {item: k for k, item in enumerate(pieces)}
    sent_to, seen = [0], [0]

    def send_piece(w, r, h):
        if r == 0 and h == 0:
            loads[w].wait()
        for way in ways(w, r):
            at = chip if r == 0 else source(way, r - 1)
            ref = slot(w, at, parity, h)
            send(ref, ref, ring_send.at[w], ring_recv.at[where[w, r, h] % SLOTS], neighbours[way])
        if r == 0 and h == parts - 1 and w < SO:
            send(own(w), own(w), sib_send.at[w], sib_recv.at[w], sibling)

    def feed():
        while sent_to[0] < len(pieces) and sent_to[0] <= seen[0] + AHEAD:
            w, r, h = pieces[sent_to[0]]
            if r > 0 and where[w, r - 1, h] >= seen[0]:
                break
            send_piece(w, r, h)
            sent_to[0] += 1

    def pump(count=1):
        for _ in range(count):
            if seen[0] == len(pieces):
                return
            w, r, h = pieces[seen[0]]
            landed(rows_of(w, len(ways(w, r)) * piece), ring_recv.at[seen[0] % SLOTS])
            seen[0] += 1
            feed()
            for way in ways(w, r) if w < SO else ():
                ref = slot(w, source(way, r), parity, h)
                send(ref, ref, sib_send.at[w], sib_recv.at[w], sibling)

    def until(w, r):
        pump(max(0, where[w, r, parts - 1] + 1 - seen[0]))

    def finish(w):
        until(w, last_round)
        landed(rows_of(w, pairs * shard), sib_recv.at[w])

    feed()
    rest[0].wait()
    rest[1].wait()

    def normalize(x):
        x = x.astype(F32)
        scale = lax.rsqrt(jnp.mean(x * x, axis=-1, keepdims=True) + 1e-06)
        return (x * scale * gain[...]).astype(BF16)

    def norm(j, carry):
        at = pl.multiple_of(j * 32, 32)
        normed[pl.ds(HALO + at, 32), :] = normalize(tokens[pl.ds(at, 32), :])
        return carry

    lax.fori_loop(0, rows // 32, norm, 0)
    for copy in rest[2:]:
        copy.wait()
    pump()
    perm = permutation(rows)
    prepare_rates(step_rate, rate)
    pump()
    prepare_inverse(decay, frequency, group, inverse)
    pump()
    prepare_inputs(inverse, input_real, input_imag, in_r, in_i)
    pump()
    base = prepare_base(log_step, decay.shape[0])
    coef[0:1, :], coef[1:2, :] = flatten([base * decay[...], base * frequency[...] * 0.15915494309189535], states)
    pump()
    opening[0:1, :], opening[1:2, :] = flatten([initial[0 : decay.shape[0], :], initial[decay.shape[0] :, :]], states)
    pump()
    rd_r[...] = read_real[...].astype(BF16)
    rd_i[...] = read_imag[...].astype(BF16)
    prepare_skip(skip_gain, skip)
    finish(S)

    def project(w):
        return dot(normed[HALO:, :], full[w]).astype(BF16)

    def project_more(w):
        return dot(normed[...], full[w]).astype(BF16)

    send(tokens.at[pl.ds(rows - SUB, SUB), :], halo, halo_send, halo_recv, after)
    state_p[...] = dot(perm, project(S)).astype(BF16)
    pump(2)
    width = min(128, channels)
    span = width // group * states
    blocks = channels // width
    for block in range(blocks):
        couple(block, state_p[:, block * width : (block + 1) * width], in_r, in_i, hr, hi, group, states)
        scan_block(block * span, span, rate, coef, hr, hi, ar, ai)
        pump(1 + block % 2)
    chain_subs(hr, hi, ar, ai, pre, level.at[0])

    def meet(k):
        landed(near.at[k], near_recv.at[k])
        mine_k, theirs = level[k], near[k]
        level[k + 1] = join(jnp.where(late[k], theirs, mine_k), jnp.where(late[k], mine_k, theirs))

    middle = outer // 2

    def pass_state(start, t):
        fin_src[0:1, :], fin_src[1:2, :] = enter(level[stages], start[0:1, :], start[1:2, :])
        for d in range(1, outer if t == middle - 1 else 2):
            if t + d < outer:
                up = ((sp + d * inner) % n_sp, fs, tp)
                remote(fin_src, inbox, chain_send.at[d - 1], chain_recv, up).start()

    def carry_low(t):
        @pl.when(layer == t)
        def _():
            if t > 0:
                landed(inbox, chain_recv)
            pass_state(inbox if t > 0 else opening, t)

    def carry_high(t):
        @pl.when(layer == t)
        def _():
            if t == middle:
                reach_map[...] = level[stages]
            else:
                landed(passed, map_recv)
                reach_map[...] = join(passed[...], level[stages])
            if t < outer - 1:
                remote(reach_map, passed, map_send, map_recv, above).start()

    for k in range(stages):
        send(level.at[k], near.at[k], near_send.at[k], near_recv.at[k], near_peers[k])
        pump(2 + k)
        meet(k)
    carry_low(0)
    carry_high(middle)
    pump(2)
    landed(halo, halo_recv)
    normed[:HALO, :] = jnp.concatenate([jnp.zeros((HALO - SUB, halo.shape[1]), BF16), normalize(halo[...])], axis=0)
    finish(V)
    value = project_more(V)
    pump(2)
    for t in range(1, middle):
        carry_low(t)
        carry_high(middle + t)
        pump(3)
    last = layer == outer - 1

    @pl.when(layer >= middle)
    def _():
        landed(inbox, chain_recv)

    @pl.when(last)
    def _():
        fin_src[0:1, :], fin_src[1:2, :] = enter(reach_map, inbox[0:1, :], inbox[1:2, :])
        for s, other in enumerate(below):
            remote(fin_src, fin_dst, fin_send.at[s], fin_recv, (other, fs, tp)).start()

    e_r = jnp.where(layer == 0, opening[0:1, :], inbox[0:1, :])
    e_i = jnp.where(layer == 0, opening[1:2, :], inbox[1:2, :])
    t_r, t_i = enter(passed, e_r, e_i)
    e_r, e_i = jnp.where(layer > middle, t_r, e_r), jnp.where(layer > middle, t_i, e_i)
    for k in reversed(range(stages)):
        t_r, t_i = enter(near[k], e_r, e_i)
        e_r, e_i = jnp.where(late[k], t_r, e_r), jnp.where(late[k], t_i, e_i)
    for block in range(blocks):
        readout(block, width, state_p, (e_r, e_i), hr, hi, ar, ai, pre, rd_r, rd_i, skip, perm, state_mix.at[parity], group, states)
        if block % 2 == 1:
            pump()

    send(state_mix.at[parity], state_mix.at[parity], mix_send.at[0], mix_recv.at[0], sibling)
    until(I, last_round)
    pump(2)
    finish(I)
    product = project_more(I).astype(F32) * value.astype(F32)
    product = jnp.where(jnp.logical_and(sp == 0, iota(product.shape, 0) < HALO), 0.0, product)
    ext[...] = product.astype(BF16).astype(F32)
    pump()
    finish(O)
    outward = project(O)
    reach = taps.shape[0] - 1
    filtered = taps[0:1, :] * ext[HALO - reach : HALO - reach + rows, :]
    for tap in range(1, reach + 1):
        at = HALO - reach + tap
        filtered = filtered + taps[tap : tap + 1, :] * ext[at : at + rows, :]
    conv_mix[parity] = (outward.astype(F32) * filtered).astype(BF16)
    own_rows = rows // n_tp
    chunks = []

    def columns(pair, par):
        return pl.ds(pl.multiple_of((pair * 2 + par) * shard, shard), shard)

    def out_rows(pairs_now, mixes):
        weights = [jnp.concatenate([full[w, columns(pair, parity), :] for pair in pairs_now], axis=0) for w in (SO, CO)]
        return sum(dot(mix, w, ((1,), (1,))) for mix, w in zip(mixes, weights)).astype(BF16)

    def compute(some):
        total = out_rows(some, [mix[...].reshape(2 * rows, mix.shape[2]) for mix in (state_mix, conv_mix)])
        for k, pair in enumerate(some):
            partial[pl.ds(pair, 1)] = total[:, k * shard : (k + 1) * shard][None]

    def compute_core(some, core):
        total = out_rows(some, [state_mix[core], conv_mix[core]])
        for k, pair in enumerate(some):
            partial[pair, pl.ds(pl.multiple_of(core * rows, rows), rows), :] = total[:, k * shard : (k + 1) * shard]

    def compute_share(pair, t):
        at = pl.ds(pl.multiple_of(t * own_rows, own_rows), own_rows)
        total = out_rows([pair], [mix[:, at, :].reshape(2 * own_rows, mix.shape[2]) for mix in (state_mix, conv_mix)])
        for core in range(2):
            spot = pl.ds(pl.multiple_of(core * rows + t * own_rows, own_rows), own_rows)
            partial[pair, spot, :] = total[core * own_rows : (core + 1) * own_rows, :]

    def exchange(pair, cores=(0, 1), shares=None):
        if all(pair is not done for done in chunks):
            chunks.append(pair)
        order = [pair is done for done in chunks].index(True)
        for s in range(n_tp) if shares is None else shares:
            for core in cores:
                if s + core > 0:
                    other = (tp + s) % n_tp
                    at = (parity if core == 0 else 1 - parity) * rows + other * own_rows
                    theirs = partial.at[pair, pl.ds(pl.multiple_of(at, own_rows), own_rows), :]
                    to = across[s] if core else (sp, fs, other)
                    send(theirs, got.at[pair, core * (n_tp - 1) + s - 1 + core], x_send, x_recv.at[order], to)

    first = [source(way, 0) for way in ways(SO, 0)]
    compute_core([chip], parity)
    send(conv_mix.at[parity], conv_mix.at[parity], mix_send.at[1], mix_recv.at[1], sibling)
    exchange(chip, cores=(0,))
    until(SO, 0)
    until(CO, 0)
    compute_core(first, parity)
    for pair in first:
        exchange(pair, cores=(0,))
    pump()
    for k, mix in enumerate((state_mix, conv_mix)):
        landed(mix.at[1 - parity], mix_recv.at[k])
    compute_core([chip], 1 - parity)
    exchange(chip, cores=(1,))
    pump()
    compute_core(first, 1 - parity)
    for pair in first:
        exchange(pair, cores=(1,))
    pump()
    for r in range(1, last_round):
        until(SO, r)
        until(CO, r)
        fresh = [source(way, r) for way in ways(SO, r)]
        compute(fresh)
        for pair in fresh:
            exchange(pair)
        pump()
    until(SO, last_round)
    until(CO, last_round)
    final_pair = source(0, last_round)
    for s in (*range(1, n_tp), 0):
        compute_share(final_pair, (tp + s) % n_tp)
        exchange(final_pair, shares=(s,))

    @pl.when(jnp.logical_not(last))
    def _():
        landed(fin_dst, fin_recv)

    share_states = states // n_sp
    groups = decay.shape[0]
    for k in range(2):
        row = jnp.where(last, fin_src[k : k + 1, :], fin_dst[k : k + 1, :])
        final[k] = own_states(row, sp, share_states, groups, states)
    kept = pl.ds(pl.multiple_of(parity * rows + tp * own_rows, own_rows), own_rows)

    def settle(k):
        ours, theirs = partial[k, kept, :].astype(F32), got[k, n_tp - 1].astype(F32)
        for s in range(1, n_tp):
            ours = ours + got[k, s - 1].astype(F32)
            theirs = theirs + got[k, n_tp - 1 + s].astype(F32)
        return ours.astype(BF16), theirs.astype(BF16)

    for c, pair in enumerate(chunks):
        landed(got.at[pair], x_recv.at[c])
        if shard % 128 == 0:
            out[:, columns(pair, parity)], out[:, columns(pair, 1 - parity)] = settle(pair)
    if shard % 128:
        for k in range(pairs):
            ours, theirs = settle(k)
            out[:, k * 2 * shard : (k * 2 + 1) * shard] = jnp.where(parity == 0, ours, theirs)
            out[:, (k * 2 + 1) * shard : (k + 1) * 2 * shard] = jnp.where(parity == 0, theirs, ours)
    for w in range(6):
        gone(rows_of(w, (pairs - 1) * shard), ring_send.at[w])
        if w < SO:
            gone(rows_of(w, pairs * shard), sib_send.at[w])
    for k in range(stages):
        gone(near.at[k], near_send.at[k])
    gone(halo, halo_send)
    gone(got, x_send)
    for k, mix in enumerate((state_mix, conv_mix)):
        gone(mix.at[parity], mix_send.at[k])

    for d in range(1, outer):
        senders = layer < middle if d == 1 else layer == middle - 1
        if d < outer - middle + 1:

            @pl.when(senders)
            def _():
                gone(fin_src, chain_send.at[d - 1])

    if outer - 1 > middle:

        @pl.when(jnp.logical_and(layer >= middle, layer < outer - 1))
        def _():
            gone(reach_map, map_send)

    for s in range(outer - 1):

        @pl.when(last)
        def _():
            gone(fin_src, fin_send.at[s])


def body(tokens, norm_gain, w_state_in, w_value, w_outer, w_inner, w_state_out, w_conv_out, log_step, decay_real, frequency, step_rate, input_real, input_imag, read_real, read_imag, skip_gain, conv_taps, initial_state):
    rows, features = tokens.shape[1:]
    groups, states = decay_real.shape
    group = skip_gain.shape[1]
    flat = groups * states
    channels = groups * group
    conv = conv_taps.shape[1]
    n_sp, n_fs, n_tp = (lax.axis_size(a) for a in ("sp", "fs", "tp"))
    shard = w_state_in.shape[0]
    pairs = n_sp * n_fs // 2
    half = pairs // 2
    inner = math.gcd(n_sp, 4)
    outer = n_sp // inner
    share = states // n_sp
    parts = pieces_of(shard)
    weights = (w_state_in, w_value, w_inner, w_outer, w_state_out, w_conv_out)
    rest = (
        tokens[0], norm_gain[None], log_step[None], decay_real, frequency, step_rate,
        jnp.swapaxes(input_real, 1, 2).reshape(channels, states), jnp.swapaxes(input_imag, 1, 2).reshape(channels, states),
        read_real.reshape(channels, states), read_imag.reshape(channels, states), skip_gain.T, conv_taps,
        initial_state.reshape(2 * groups, states),
    )
    vmem = pltpu.VMEM
    dma = pltpu.SemaphoreType.DMA
    out, final = pl.pallas_call(
        lambda *refs: layer_kernel((n_sp, n_fs, n_tp, group, states), *refs),
        out_shape=(jax.ShapeDtypeStruct((rows // n_tp, features), BF16), jax.ShapeDtypeStruct((2, share, groups), F32)),
        in_specs=[pl.BlockSpec(memory_space=pltpu.HBM)] * 19,
        out_specs=[pl.BlockSpec(memory_space=vmem)] * 2,
        scratch_shapes=[
            *[vmem(a.shape, a.dtype) for a in rest],
            vmem((6, n_sp * n_fs * shard, channels), BF16),
            vmem((HALO + rows, features), BF16),
            vmem((rows, channels), BF16),
            *[vmem((rows, flat), F32)] * 4,
            vmem((4, SUB, flat), F32),
            vmem((inner.bit_length(), 4, flat), F32),
            vmem((inner.bit_length() - 1, 4, flat), F32),
            vmem((2, flat), F32),
            vmem((4, flat), F32),
            vmem((4, flat), F32),
            vmem((2, flat), F32),
            vmem((2, flat), F32),
            vmem((rows + HALO, conv), F32),
            vmem((SUB, features), BF16),
            vmem((2, rows, conv), BF16),
            vmem((2, rows, channels), BF16),
            vmem((pairs, 2 * rows, shard), BF16),
            vmem((pairs, 2 * n_tp - 1, rows // n_tp, shard), BF16),
            vmem((rows, 128), F32),
            vmem((2, flat), F32),
            vmem((2, flat), F32),
            *[vmem((channels, states), BF16)] * 4,
            vmem((1, channels), F32),
            vmem((2, channels, states), F32),
            dma((13,)),
            dma((6,)),
            dma((6,)),
            dma((SLOTS,)),
            dma((SO,)),
            dma((SO,)),
            dma((inner.bit_length() - 1,)),
            dma((inner.bit_length() - 1,)),
            dma((outer - 1,)),
            dma,
            dma,
            dma,
            dma((outer - 1,)),
            dma,
            dma,
            dma((pairs,)),
            dma,
            dma,
            dma((2,)),
            dma((2,)),
        ],
        compiler_params=pltpu.CompilerParams(collective_id=0, has_side_effects=True, vmem_limit_bytes=36 * 1024 * 1024),
        name="layer",
    )(*(pltpu.with_memory_space_constraint(a, pltpu.HBM) for a in weights + rest))
    return out[None], jnp.swapaxes(final, 1, 2)[None]


def solution(mesh):
    return jax.shard_map(
        body,
        mesh=mesh,
        in_specs=(
            P("fs", "sp", None),
            P(),
            P(("sp", "fs"), "tp"),
            P(("sp", "fs"), "tp"),
            P(("sp", "fs"), "tp"),
            P(("sp", "fs"), "tp"),
            P(("sp", "fs"), "tp"),
            P(("sp", "fs"), "tp"),
            P("tp"),
            P("tp", None),
            P("tp", None),
            P("fs", "sp"),
            P("tp", None, None),
            P("tp", None, None),
            P("tp", None, None),
            P("tp", None, None),
            P("tp", None),
            P(None, "tp"),
            P("fs", None, "tp", None),
        ),
        out_specs=(P("fs", ("sp", "tp"), None), P("fs", None, "tp", "sp")),
        check_vma=False,
    )
```

```python
import math

import jax
import jax.numpy as jnp
from jax import lax
from jax.experimental import pallas as pl
from jax.experimental.pallas import tpu as pltpu
from jax.sharding import PartitionSpec as P

F32 = jnp.float32
BF16 = jnp.bfloat16
SUB = 8
SIN = (3.1415925798055846, -5.16770686616794, 2.5500311935192803, -0.5980441939118888, 0.07721838615680923)
COS = (0.9999999997799038, -4.93480213707883, 4.058709159556464, -1.335212003052184, 0.2349373138245546, -0.024396324364378108)


def poly(coeffs, z):
    total = coeffs[-1]
    for c in coeffs[-2::-1]:
        total = total * z + c
    return total


def dot(a, b, dims=((1,), (0,))):
    return lax.dot_general(a, b, (dims, ((), ())), preferred_element_type=F32)


def iota(shape, dim):
    return lax.broadcasted_iota(jnp.int32, shape, dim)


def exact(a, b, dims=((1,), (0,))):
    return lax.dot_general(a, b, (dims, ((), ())), precision=lax.Precision.HIGHEST, preferred_element_type=F32)


def cmul(ar, ai, br, bi):
    return ar * br - ai * bi, ar * bi + ai * br


def permutation(rows):
    run = rows // SUB
    r, t = iota((rows, rows), 0), iota((rows, rows), 1)
    return jnp.where((r % SUB) * run + r // SUB == t, 1.0, 0.0).astype(BF16)


def spread(mat, block, width, span, group, states):
    chans = slice(block * width, (block + 1) * width)
    tile = jnp.where(iota((states, span), 0) == iota((states, span), 1) % states, 1.0, 0.0).astype(BF16)
    keep = iota((width, span), 0) // group == iota((width, span), 1) // states
    return jnp.where(keep, dot(mat[chans, :], tile), 0.0).astype(BF16)


def couple(block, state_p, in_r, in_i, dr_ref, di_ref, group, states):
    width = state_p.shape[1]
    span = width // group * states
    cols = slice(block * span, (block + 1) * span)
    for src, dst in ((in_r, dr_ref), (in_i, di_ref)):
        dst[:, cols] = dot(state_p, spread(src, block, width, span, group, states))


def scan_block(lo, span, rate, coef, hr, hi, ar, ai):
    cols = pl.ds(lo, span)
    run = rate.shape[0] // SUB
    reps = span // 128
    decay = jnp.broadcast_to(coef[0:1, cols], (SUB, span))
    turn = jnp.broadcast_to(coef[1:2, cols], (SUB, span))

    def one(j, carry):
        h_r, h_i, a_r, a_i = carry
        at = pl.ds(pl.multiple_of(j * SUB, SUB), SUB)
        r = jnp.concatenate([rate[at, :]] * reps, axis=1)
        u = r * turn
        f = u - jnp.floor(u + 0.5)
        z = f * f
        s = f * poly(SIN, z)
        c = poly(COS, z)
        grow = jnp.exp(r * decay)
        gs = 2.0 * grow * s
        b_r = grow - gs * s
        b_i = gs * c
        p_r, p_i = cmul(b_r - 1.0, b_i, hr[at, cols], hi[at, cols])
        m_r, m_i = cmul(b_r, b_i, h_r, h_i)
        h_r, h_i = m_r + p_r, m_i + p_i
        a_r, a_i = cmul(b_r, b_i, a_r, a_i)
        hr[at, cols] = h_r
        hi[at, cols] = h_i
        ar[at, cols] = a_r
        ai[at, cols] = a_i
        return h_r, h_i, a_r, a_i

    zero = jnp.zeros((SUB, span), F32)
    lax.fori_loop(0, run, one, (zero, zero, zero + 1.0, zero), unroll=2)


def chain_subs(hr, hi, ar, ai, pre, summ):
    rows, flat = hr.shape
    last = rows - SUB
    m_r, m_i = jnp.ones((1, flat), F32), jnp.zeros((1, flat), F32)
    v_r, v_i = jnp.zeros((1, flat), F32), jnp.zeros((1, flat), F32)
    for s in range(SUB):
        row = slice(s, s + 1)
        pre[0, row, :], pre[1, row, :], pre[2, row, :], pre[3, row, :] = m_r, m_i, v_r, v_i
        at = slice(last + s, last + s + 1)
        e_r, e_i = ar[at, :], ai[at, :]
        m_r, m_i = cmul(e_r, e_i, m_r, m_i)
        w_r, w_i = cmul(e_r, e_i, v_r, v_i)
        v_r, v_i = w_r + hr[at, :], w_i + hi[at, :]
    summ[0:1, :], summ[1:2, :], summ[2:3, :], summ[3:4, :] = m_r, m_i, v_r, v_i


def enter(g, s_r, s_i):
    t_r, t_i = cmul(g[0:1, :], g[1:2, :], s_r, s_i)
    return t_r + g[2:3, :], t_i + g[3:4, :]


def join(first, second):
    g_r, g_i = second[0:1, :], second[1:2, :]
    m_r, m_i = cmul(g_r, g_i, first[0:1, :], first[1:2, :])
    w_r, w_i = cmul(g_r, g_i, first[2:3, :], first[3:4, :])
    return jnp.concatenate([m_r, m_i, w_r + second[2:3, :], w_i + second[3:4, :]], axis=0)


def readout(block, width, state_p, enter, hr, hi, ar, ai, pre, rd_r, rd_i, skip, perm, out, group, states):
    span = width // group * states
    cols = slice(block * span, (block + 1) * span)
    chans = slice(block * width, (block + 1) * width)
    rows = hr.shape[0]
    run = rows // SUB
    e_r, e_i = cmul(pre[0, :, cols], pre[1, :, cols], enter[0][:, cols], enter[1][:, cols])
    e_r, e_i = e_r + pre[2, :, cols], e_i + pre[3, :, cols]
    g_r = spread(rd_r, block, width, span, group, states)
    g_i = spread(rd_i, block, width, span, group, states)

    def fixed(local, a, b, sign):
        a3, b3 = a[:, cols].reshape(run, SUB, span), b[:, cols].reshape(run, SUB, span)
        x, y = (e_r, e_i) if sign < 0 else (e_i, e_r)
        shift = a3 * x[None] + (b3 * y[None] if sign > 0 else -b3 * y[None])
        return (local[:, cols].reshape(run, SUB, span) + shift).reshape(rows, span).astype(BF16)

    total = dot(fixed(hr, ar, ai, -1), g_r, ((1,), (1,))) - dot(fixed(hi, ar, ai, 1), g_i, ((1,), (1,)))
    v = total + skip[:, chans] * state_p[:, chans].astype(F32)
    mix = 0.5 * v * (1.0 + jnp.tanh(0.7978845608 * (v + 0.044715 * (v * v * v))))
    out[:, chans] = dot(perm, mix.astype(BF16), ((0,), (0,))).astype(BF16)


def prepare_rates(step_rate, rate):
    rows = rate.shape[0]
    run = rows // SUB
    r, t = iota((rows, rows), 0), iota((rows, rows), 1)
    chosen = jnp.where((r % SUB) * run + r // SUB == t, jnp.broadcast_to(step_rate[...], (rows, rows)), 0.0)
    rate[...] = exact(chosen, jnp.ones((rows, 128), F32))


def flatten(parts, states):
    groups = parts[0].shape[0]
    flat = groups * states
    tile = jnp.where(iota((states, flat), 0) == iota((states, flat), 1) % states, 1.0, 0.0)
    keep = iota((groups, flat), 0) == iota((groups, flat), 1) // states
    return [jnp.sum(jnp.where(keep, exact(part, tile), 0.0), axis=0, keepdims=True) for part in parts]


def prepare_base(log_step, groups):
    base = jnp.where(iota((groups, groups), 0) == iota((groups, groups), 1), jnp.broadcast_to(jnp.exp(log_step[...]), (groups, groups)), 0.0)
    return jnp.sum(base, axis=1, keepdims=True)


def prepare_inverse(decay, frequency, group, scratch):
    groups = decay.shape[0]
    d, f = decay[...], frequency[...]
    modulus = d * d + f * f
    each = jnp.where(iota((groups * group, groups), 0) // group == iota((groups * group, groups), 1), 1.0, 0.0)
    scratch[0], scratch[1] = exact(each, d / modulus), exact(each, -f / modulus)


def prepare_inputs(inverse, input_real, input_imag, in_r, in_i):
    x_r, x_i = input_real[...], input_imag[...]
    in_r[...] = (x_r * inverse[0] - x_i * inverse[1]).astype(BF16)
    in_i[...] = (x_r * inverse[1] + x_i * inverse[0]).astype(BF16)


def prepare_skip(skip_gain, skip):
    group, groups = skip_gain.shape
    chans = groups * group
    each = jnp.where(iota((groups, chans), 0) == iota((groups, chans), 1) // group, 1.0, 0.0)
    keep = iota((group, chans), 0) == iota((group, chans), 1) % group
    skip[...] = jnp.sum(jnp.where(keep, exact(skip_gain[...], each), 0.0), axis=0, keepdims=True)


def own_states(row, sp, share, groups, states):
    flat = groups * states
    shape = (SUB, flat)
    mine = jnp.where(iota(shape, 1) % states == sp * share + iota(shape, 0), jnp.broadcast_to(row, shape), 0.0)
    each = jnp.where(iota((groups, flat), 0) == iota((groups, flat), 1) // states, 1.0, 0.0)
    return exact(mine, each, ((1,), (1,)))[0:share, :]


MESH = pl.DeviceIdType.MESH
HALO = 16
AHEAD = 5
SLOTS = 16


def pieces_of(shard):
    return 2 if shard >= 64 else 1


S, V, I, O, SO, CO = range(6)


def layer_kernel(sizes, *refs):
    n_sp, n_fs, n_tp, group, states = sizes
    inputs, (out, final), scratch = refs[:19], refs[19:21], refs[21:]
    hbm_weights, hbm_rest = inputs[:6], inputs[6:]
    local, scratch = scratch[:13], scratch[13:]
    (
        full, normed, state_p, hr, hi, ar, ai, pre, level, near, inbox, passed, reach_map, fin_src, fin_dst, ext, halo,
        conv_mix, state_mix, partial, got, rate, coef, opening, in_r, in_i, rd_r, rd_i, skip, inverse,
        load, load_w, ring_send, ring_recv, sib_send, sib_recv, near_send, near_recv, chain_send, chain_recv, map_send, map_recv, fin_send, fin_recv,
        x_send, x_recv, halo_send, halo_recv, mix_send, mix_recv,
    ) = scratch
    tokens, gain, log_step, decay, frequency, step_rate, input_real, input_imag, read_real, read_imag, skip_gain, taps, initial = local
    shard = hbm_weights[0].shape[0]
    rows = tokens.shape[0]
    channels = hbm_weights[0].shape[1]
    sp, fs, tp = lax.axis_index("sp"), lax.axis_index("fs"), lax.axis_index("tp")
    pairs = n_sp * n_fs // 2
    half = pairs // 2
    parts = pieces_of(shard)
    piece = shard // parts
    inner = math.gcd(n_sp, 4)
    outer = n_sp // inner
    here, layer = sp % inner, sp // inner
    mine = sp * n_fs + fs
    parity, chip = mine % 2, mine // 2
    place = jnp.where(chip % 2 == 0, chip // 2, pairs - 1 - chip // 2)

    def own(w):
        return full.at[w, pl.ds(pl.multiple_of(mine * shard, shard), shard), :]

    loads = [pltpu.make_async_copy(src, own(w), load_w.at[w]) for w, src in enumerate(hbm_weights)]
    rest = [pltpu.make_async_copy(src, dst, load.at[k]) for k, (src, dst) in enumerate(zip(hbm_rest, local))]
    for copy in loads[:2] + rest[:1] + loads[2:] + rest[1:]:
        copy.start()

    def pair_at(offset):
        q = (place + offset + pairs) % pairs
        return jnp.where(q < half, q * 2, (pairs - 1 - q) * 2 + 1)

    def device(linear):
        return (linear // n_fs, linear % n_fs, tp)

    neighbours = (device(pair_at(1) * 2 + parity), device(pair_at(-1) * 2 + parity))
    sibling = device(chip * 2 + 1 - parity)
    stages = inner.bit_length() - 1
    late = [(here >> k) % 2 == 1 for k in range(stages)]
    near_peers = [(sp + jnp.where(late[k], -1, 1) * (1 << k), fs, tp) for k in range(stages)]
    above = ((sp + inner) % n_sp, fs, tp)
    below = [(sp - s * inner + n_sp) % n_sp for s in range(1, outer)]
    after = ((sp + 1) % n_sp, fs, tp)
    tp_peers = [(sp, fs, (tp + s) % n_tp) for s in range(1, n_tp)]

    barrier = pltpu.get_barrier_semaphore()
    across = [(sibling[0], sibling[1], (tp + s) % n_tp) for s in range(n_tp)]
    greet = list(neighbours) + tp_peers + across
    for other in greet:
        pl.semaphore_signal(barrier, inc=1, device_id=other, device_id_type=MESH)
    pl.semaphore_wait(barrier, len(greet))

    def remote(src, dst, s_sem, r_sem, to):
        return pltpu.make_async_remote_copy(src_ref=src, dst_ref=dst, send_sem=s_sem, recv_sem=r_sem, device_id=to, device_id_type=MESH)

    def send(src, dst, s_sem, r_sem, to):
        remote(src, dst, s_sem, r_sem, to).start()

    def landed(ref, r_sem):
        remote(ref, ref, r_sem, r_sem, sibling).wait_recv()

    def gone(ref, s_sem):
        remote(ref, ref, s_sem, s_sem, sibling).wait_send()

    def slot(w, pair, par, h):
        return full.at[w, pl.ds(pl.multiple_of((pair * 2 + par) * shard + h * piece, piece), piece), :]

    def rounds(w, way):
        return half if way == w % 2 else pairs - 1 - half

    def source(way, r):
        return pair_at(-1 - r if way == 0 else 1 + r)

    def ways(w, r):
        return [way for way in range(2) if r < rounds(w, way)]

    def rows_of(w, count):
        return full.at[w, pl.ds(0, count), :]

    last_round = half - 1
    filler = [(V, r, h) for r in range(half) for h in range(parts)]
    pieces = []
    for r in range(half):
        pieces += [(S, r, h) for h in range(parts)] + filler[:1]
        del filler[:1]
    outputs = [(w, r) for r in range(half) for w in (SO, CO)]

    def both(*units):
        return [(w, r, h) for w, r in units for h in range(parts)]

    for r in range(half):
        if r < last_round:
            pieces += both((I, r), (O, r)) + filler[:parts]
            del filler[:parts]
        else:
            pieces += filler + both(outputs[0], (I, r), (O, r), *outputs[1:])
    where = {item: k for k, item in enumerate(pieces)}
    sent_to, seen = [0], [0]

    def send_piece(w, r, h):
        if r == 0 and h == 0:
            loads[w].wait()
        for way in ways(w, r):
            at = chip if r == 0 else source(way, r - 1)
            ref = slot(w, at, parity, h)
            send(ref, ref, ring_send, ring_recv.at[where[w, r, h] % SLOTS], neighbours[way])
        if r == 0 and h == parts - 1 and w < SO:
            send(own(w), own(w), sib_send, sib_recv.at[w], sibling)

    def feed():
        while sent_to[0] < len(pieces) and sent_to[0] <= seen[0] + AHEAD:
            w, r, h = pieces[sent_to[0]]
            if r > 0 and where[w, r - 1, h] >= seen[0]:
                break
            send_piece(w, r, h)
            sent_to[0] += 1

    def pump(count=1):
        for _ in range(count):
            if seen[0] == len(pieces):
                return
            w, r, h = pieces[seen[0]]
            landed(rows_of(w, len(ways(w, r)) * piece), ring_recv.at[seen[0] % SLOTS])
            seen[0] += 1
            feed()
            for way in ways(w, r) if w < SO else ():
                ref = slot(w, source(way, r), parity, h)
                send(ref, ref, sib_send, sib_recv.at[w], sibling)

    def until(w, r):
        pump(max(0, where[w, r, parts - 1] + 1 - seen[0]))

    def finish(w):
        until(w, last_round)
        landed(rows_of(w, pairs * shard), sib_recv.at[w])

    feed()
    rest[0].wait()
    rest[1].wait()

    def normalize(x):
        x = x.astype(F32)
        scale = lax.rsqrt(jnp.mean(x * x, axis=-1, keepdims=True) + 1e-06)
        return (x * scale * gain[...]).astype(BF16)

    def norm(j, carry):
        at = pl.multiple_of(j * 32, 32)
        normed[pl.ds(HALO + at, 32), :] = normalize(tokens[pl.ds(at, 32), :])
        return carry

    lax.fori_loop(0, rows // 32, norm, 0)
    for copy in rest[2:]:
        copy.wait()
    pump()
    perm = permutation(rows)
    prepare_rates(step_rate, rate)
    pump()
    prepare_inverse(decay, frequency, group, inverse)
    pump()
    prepare_inputs(inverse, input_real, input_imag, in_r, in_i)
    pump()
    base = prepare_base(log_step, decay.shape[0])
    coef[0:1, :], coef[1:2, :] = flatten([base * decay[...], base * frequency[...] * 0.15915494309189535], states)
    pump()
    opening[0:1, :], opening[1:2, :] = flatten([initial[0 : decay.shape[0], :], initial[decay.shape[0] :, :]], states)
    pump()
    rd_r[...] = read_real[...].astype(BF16)
    rd_i[...] = read_imag[...].astype(BF16)
    prepare_skip(skip_gain, skip)
    finish(S)

    def project(w):
        return dot(normed[HALO:, :], full[w]).astype(BF16)

    def project_more(w):
        return dot(normed[...], full[w]).astype(BF16)

    send(tokens.at[pl.ds(rows - SUB, SUB), :], halo, halo_send, halo_recv, after)
    state_p[...] = dot(perm, project(S)).astype(BF16)
    pump(2)
    width = min(128, channels)
    span = width // group * states
    blocks = channels // width
    for block in range(blocks):
        couple(block, state_p[:, block * width : (block + 1) * width], in_r, in_i, hr, hi, group, states)
        scan_block(block * span, span, rate, coef, hr, hi, ar, ai)
        pump(1 + block % 2)
    chain_subs(hr, hi, ar, ai, pre, level.at[0])

    def meet(k):
        landed(near.at[k], near_recv.at[k])
        mine_k, theirs = level[k], near[k]
        level[k + 1] = join(jnp.where(late[k], theirs, mine_k), jnp.where(late[k], mine_k, theirs))

    middle = outer // 2

    def pass_state(start, t):
        fin_src[0:1, :], fin_src[1:2, :] = enter(level[stages], start[0:1, :], start[1:2, :])
        for d in range(1, outer if t == middle - 1 else 2):
            if t + d < outer:
                up = ((sp + d * inner) % n_sp, fs, tp)
                remote(fin_src, inbox, chain_send.at[d - 1], chain_recv, up).start()

    def carry_low(t):
        @pl.when(layer == t)
        def _():
            if t > 0:
                landed(inbox, chain_recv)
            pass_state(inbox if t > 0 else opening, t)

    def carry_high(t):
        @pl.when(layer == t)
        def _():
            if t == middle:
                reach_map[...] = level[stages]
            else:
                landed(passed, map_recv)
                reach_map[...] = join(passed[...], level[stages])
            if t < outer - 1:
                remote(reach_map, passed, map_send, map_recv, above).start()

    for k in range(stages):
        send(level.at[k], near.at[k], near_send.at[k], near_recv.at[k], near_peers[k])
        pump(2 + k)
        meet(k)
    carry_low(0)
    carry_high(middle)
    pump(2)
    landed(halo, halo_recv)
    normed[:HALO, :] = jnp.concatenate([jnp.zeros((HALO - SUB, halo.shape[1]), BF16), normalize(halo[...])], axis=0)
    finish(V)
    value = project_more(V)
    pump(2)
    for t in range(1, middle):
        carry_low(t)
        carry_high(middle + t)
        pump(3)
    last = layer == outer - 1

    @pl.when(layer >= middle)
    def _():
        landed(inbox, chain_recv)

    @pl.when(last)
    def _():
        fin_src[0:1, :], fin_src[1:2, :] = enter(reach_map, inbox[0:1, :], inbox[1:2, :])
        for s, other in enumerate(below):
            remote(fin_src, fin_dst, fin_send.at[s], fin_recv, (other, fs, tp)).start()

    e_r = jnp.where(layer == 0, opening[0:1, :], inbox[0:1, :])
    e_i = jnp.where(layer == 0, opening[1:2, :], inbox[1:2, :])
    t_r, t_i = enter(passed, e_r, e_i)
    e_r, e_i = jnp.where(layer > middle, t_r, e_r), jnp.where(layer > middle, t_i, e_i)
    for k in reversed(range(stages)):
        t_r, t_i = enter(near[k], e_r, e_i)
        e_r, e_i = jnp.where(late[k], t_r, e_r), jnp.where(late[k], t_i, e_i)
    for block in range(blocks):
        readout(block, width, state_p, (e_r, e_i), hr, hi, ar, ai, pre, rd_r, rd_i, skip, perm, state_mix.at[parity], group, states)
        if block % 2 == 1:
            pump()

    send(state_mix.at[parity], state_mix.at[parity], mix_send.at[0], mix_recv.at[0], sibling)
    until(I, last_round)
    pump(2)
    finish(I)
    product = project_more(I).astype(F32) * value.astype(F32)
    product = jnp.where(jnp.logical_and(sp == 0, iota(product.shape, 0) < HALO), 0.0, product)
    ext[...] = product.astype(BF16).astype(F32)
    pump()
    finish(O)
    outward = project(O)
    reach = taps.shape[0] - 1
    filtered = taps[0:1, :] * ext[HALO - reach : HALO - reach + rows, :]
    for tap in range(1, reach + 1):
        at = HALO - reach + tap
        filtered = filtered + taps[tap : tap + 1, :] * ext[at : at + rows, :]
    conv_mix[parity] = (outward.astype(F32) * filtered).astype(BF16)
    own_rows = rows // n_tp
    chunks = []

    def columns(pair, par):
        return pl.ds(pl.multiple_of((pair * 2 + par) * shard, shard), shard)

    def out_rows(pairs_now, mixes):
        weights = [jnp.concatenate([full[w, columns(pair, parity), :] for pair in pairs_now], axis=0) for w in (SO, CO)]
        return sum(dot(mix, w, ((1,), (1,))) for mix, w in zip(mixes, weights)).astype(BF16)

    def out_part(some, mix, w):
        weight = jnp.concatenate([full[w, columns(pair, parity), :] for pair in some], axis=0)
        return dot(mix[...].reshape(2 * rows, mix.shape[2]), weight, ((1,), (1,)))

    def compute(some, state_part):
        total = (state_part + out_part(some, conv_mix, CO)).astype(BF16)
        for k, pair in enumerate(some):
            partial[pl.ds(pair, 1)] = total[:, k * shard : (k + 1) * shard][None]

    def compute_core(some, core):
        total = out_rows(some, [state_mix[core], conv_mix[core]])
        for k, pair in enumerate(some):
            partial[pair, pl.ds(pl.multiple_of(core * rows, rows), rows), :] = total[:, k * shard : (k + 1) * shard]

    def share_rows(mix, t):
        at = pl.ds(pl.multiple_of(t * own_rows, own_rows), own_rows)
        return mix[:, at, :].reshape(2 * own_rows, mix.shape[2])

    def finish_share(pair, t, state_part):
        total = (state_part + dot(share_rows(conv_mix, t), full[CO, columns(pair, parity), :], ((1,), (1,)))).astype(BF16)
        for core in range(2):
            spot = pl.ds(pl.multiple_of(core * rows + t * own_rows, own_rows), own_rows)
            partial[pair, spot, :] = total[core * own_rows : (core + 1) * own_rows, :]

    def exchange(pair, cores=(0, 1), shares=None):
        if all(pair is not done for done in chunks):
            chunks.append(pair)
        order = [pair is done for done in chunks].index(True)
        for s in range(n_tp) if shares is None else shares:
            for core in cores:
                if s + core > 0:
                    other = (tp + s) % n_tp
                    at = (parity if core == 0 else 1 - parity) * rows + other * own_rows
                    theirs = partial.at[pair, pl.ds(pl.multiple_of(at, own_rows), own_rows), :]
                    to = across[s] if core else (sp, fs, other)
                    send(theirs, got.at[pair, core * (n_tp - 1) + s - 1 + core], x_send, x_recv.at[order], to)

    first = [source(way, 0) for way in ways(SO, 0)]
    compute_core([chip], parity)
    send(conv_mix.at[parity], conv_mix.at[parity], mix_send.at[1], mix_recv.at[1], sibling)
    exchange(chip, cores=(0,))
    until(SO, 0)
    until(CO, 0)
    compute_core(first, parity)
    for pair in first:
        exchange(pair, cores=(0,))
    pump()
    for k, mix in enumerate((state_mix, conv_mix)):
        landed(mix.at[1 - parity], mix_recv.at[k])
    compute_core([chip], 1 - parity)
    exchange(chip, cores=(1,))
    pump()
    compute_core(first, 1 - parity)
    for pair in first:
        exchange(pair, cores=(1,))
    pump()
    for r in range(1, last_round):
        until(SO, r)
        fresh = [source(way, r) for way in ways(SO, r)]
        state_part = out_part(fresh, state_mix, SO)
        until(CO, r)
        compute(fresh, state_part)
        for pair in fresh:
            exchange(pair)
        pump()
    until(SO, last_round)
    final_pair = source(0, last_round)
    order = [(s, (tp + s) % n_tp) for s in (*range(1, n_tp), 0)]
    state_parts = [dot(share_rows(state_mix, t), full[SO, columns(final_pair, parity), :], ((1,), (1,))) for _, t in order]
    until(CO, last_round)
    for (s, t), state_part in zip(order, state_parts):
        finish_share(final_pair, t, state_part)
        exchange(final_pair, shares=(s,))

    @pl.when(jnp.logical_not(last))
    def _():
        landed(fin_dst, fin_recv)

    share_states = states // n_sp
    groups = decay.shape[0]
    for k in range(2):
        row = jnp.where(last, fin_src[k : k + 1, :], fin_dst[k : k + 1, :])
        final[k] = own_states(row, sp, share_states, groups, states)
    kept = pl.ds(pl.multiple_of(parity * rows + tp * own_rows, own_rows), own_rows)

    def settle(k):
        ours, theirs = partial[k, kept, :].astype(F32), got[k, n_tp - 1].astype(F32)
        for s in range(1, n_tp):
            ours = ours + got[k, s - 1].astype(F32)
            theirs = theirs + got[k, n_tp - 1 + s].astype(F32)
        return ours.astype(BF16), theirs.astype(BF16)

    for c, pair in enumerate(chunks):
        landed(got.at[pair], x_recv.at[c])
        if shard % 128 == 0:
            out[:, columns(pair, parity)], out[:, columns(pair, 1 - parity)] = settle(pair)
    if shard % 128:
        for k in range(pairs):
            ours, theirs = settle(k)
            out[:, k * 2 * shard : (k * 2 + 1) * shard] = jnp.where(parity == 0, ours, theirs)
            out[:, (k * 2 + 1) * shard : (k + 1) * 2 * shard] = jnp.where(parity == 0, theirs, ours)
    gone(full.at[:, pl.ds(0, (pairs - 1) * shard), :], ring_send)
    gone(full.at[pl.ds(0, SO), pl.ds(0, pairs * shard), :], sib_send)
    for k in range(stages):
        gone(near.at[k], near_send.at[k])
    gone(halo, halo_send)
    gone(got, x_send)
    for k, mix in enumerate((state_mix, conv_mix)):
        gone(mix.at[parity], mix_send.at[k])

    for d in range(1, outer):
        senders = layer < middle if d == 1 else layer == middle - 1
        if d < outer - middle + 1:

            @pl.when(senders)
            def _():
                gone(fin_src, chain_send.at[d - 1])

    if outer - 1 > middle:

        @pl.when(jnp.logical_and(layer >= middle, layer < outer - 1))
        def _():
            gone(reach_map, map_send)

    for s in range(outer - 1):

        @pl.when(last)
        def _():
            gone(fin_src, fin_send.at[s])


def body(tokens, norm_gain, w_state_in, w_value, w_outer, w_inner, w_state_out, w_conv_out, log_step, decay_real, frequency, step_rate, input_real, input_imag, read_real, read_imag, skip_gain, conv_taps, initial_state):
    rows, features = tokens.shape[1:]
    groups, states = decay_real.shape
    group = skip_gain.shape[1]
    flat = groups * states
    channels = groups * group
    conv = conv_taps.shape[1]
    n_sp, n_fs, n_tp = (lax.axis_size(a) for a in ("sp", "fs", "tp"))
    shard = w_state_in.shape[0]
    pairs = n_sp * n_fs // 2
    half = pairs // 2
    inner = math.gcd(n_sp, 4)
    outer = n_sp // inner
    share = states // n_sp
    parts = pieces_of(shard)
    weights = (w_state_in, w_value, w_inner, w_outer, w_state_out, w_conv_out)
    rest = (
        tokens[0], norm_gain[None], log_step[None], decay_real, frequency, step_rate,
        jnp.swapaxes(input_real, 1, 2).reshape(channels, states), jnp.swapaxes(input_imag, 1, 2).reshape(channels, states),
        read_real.reshape(channels, states), read_imag.reshape(channels, states), skip_gain.T, conv_taps,
        initial_state.reshape(2 * groups, states),
    )
    vmem = pltpu.VMEM
    dma = pltpu.SemaphoreType.DMA
    out, final = pl.pallas_call(
        lambda *refs: layer_kernel((n_sp, n_fs, n_tp, group, states), *refs),
        out_shape=(jax.ShapeDtypeStruct((rows // n_tp, features), BF16), jax.ShapeDtypeStruct((2, share, groups), F32)),
        in_specs=[pl.BlockSpec(memory_space=pltpu.HBM)] * 19,
        out_specs=[pl.BlockSpec(memory_space=vmem)] * 2,
        scratch_shapes=[
            *[vmem(a.shape, a.dtype) for a in rest],
            vmem((6, n_sp * n_fs * shard, channels), BF16),
            vmem((HALO + rows, features), BF16),
            vmem((rows, channels), BF16),
            *[vmem((rows, flat), F32)] * 4,
            vmem((4, SUB, flat), F32),
            vmem((inner.bit_length(), 4, flat), F32),
            vmem((inner.bit_length() - 1, 4, flat), F32),
            vmem((2, flat), F32),
            vmem((4, flat), F32),
            vmem((4, flat), F32),
            vmem((2, flat), F32),
            vmem((2, flat), F32),
            vmem((rows + HALO, conv), F32),
            vmem((SUB, features), BF16),
            vmem((2, rows, conv), BF16),
            vmem((2, rows, channels), BF16),
            vmem((pairs, 2 * rows, shard), BF16),
            vmem((pairs, 2 * n_tp - 1, rows // n_tp, shard), BF16),
            vmem((rows, 128), F32),
            vmem((2, flat), F32),
            vmem((2, flat), F32),
            *[vmem((channels, states), BF16)] * 4,
            vmem((1, channels), F32),
            vmem((2, channels, states), F32),
            dma((13,)),
            dma((6,)),
            dma,
            dma((SLOTS,)),
            dma,
            dma((SO,)),
            dma((inner.bit_length() - 1,)),
            dma((inner.bit_length() - 1,)),
            dma((outer - 1,)),
            dma,
            dma,
            dma,
            dma((outer - 1,)),
            dma,
            dma,
            dma((pairs,)),
            dma,
            dma,
            dma((2,)),
            dma((2,)),
        ],
        compiler_params=pltpu.CompilerParams(collective_id=0, has_side_effects=True, vmem_limit_bytes=36 * 1024 * 1024),
        name="layer",
    )(*(pltpu.with_memory_space_constraint(a, pltpu.HBM) for a in weights + rest))
    return out[None], jnp.swapaxes(final, 1, 2)[None]


def solution(mesh):
    return jax.shard_map(
        body,
        mesh=mesh,
        in_specs=(
            P("fs", "sp", None),
            P(),
            P(("sp", "fs"), "tp"),
            P(("sp", "fs"), "tp"),
            P(("sp", "fs"), "tp"),
            P(("sp", "fs"), "tp"),
            P(("sp", "fs"), "tp"),
            P(("sp", "fs"), "tp"),
            P("tp"),
            P("tp", None),
            P("tp", None),
            P("fs", "sp"),
            P("tp", None, None),
            P("tp", None, None),
            P("tp", None, None),
            P("tp", None, None),
            P("tp", None),
            P(None, "tp"),
            P("fs", None, "tp", None),
        ),
        out_specs=(P("fs", ("sp", "tp"), None), P("fs", None, "tp", "sp")),
        check_vma=False,
    )
```
